32 devices in a mesh: sp: 4 (over z), fs: 4 (over y, x), tp: 2 (over core).
Axes of the slice: x: 2, y: 2, z: 4, core: 2. Of those that a mesh axis runs over, the one named last changes fastest.
Arguments:
- tokens: bfloat16 [4, 2048, 2048], P('fs', ('sp', 'tp')), may hold values from -6 to 6
- norm_gain: float32 [2048], replicated, may hold values from 0.1 to 1.9
- query_weight: bfloat16 [2048, 1024], P('sp', 'tp'), may hold values from -20 to 20
- key_matrix: bfloat16 [2048, 256], P('sp', 'tp'), may hold values from -0.125 to 0.125
- value_matrix: bfloat16 [2048, 256], P('sp', 'tp'), may hold values from -0.125 to 0.125
- pool_in_weight: bfloat16 [2048, 1024], P('sp', 'tp'), may hold values from -0.125 to 0.125
- head_sink_logit: float32 [16], replicated, may hold values from 2 to 6
- pool_mix: bfloat16 [4, 256, 256], replicated, may hold values from -0.375 to 0.375
- pool_gain: float32 [1024], replicated, may hold values from 0.1 to 1.9
- attn_out_weight: bfloat16 [1024, 2048], P('tp', 'sp'), may hold values from -1 to 1
- pool_out_weight: bfloat16 [1024, 2048], P('tp', 'sp'), may hold values from -0.125 to 0.125
Outputs:
- mixed: bfloat16 [4, 2048, 2048], P('fs', ('sp', 'tp'))
- row_log_weight_sum: float32 [4, 16, 2048], P('fs', 'tp', 'sp')
The draws below stay inside these ranges and needn't reach their ends.
All inputs are finite; a program needn't handle non-finite values.
Results may differ from the reference program's by a relative error of at most 0.0095.
The reference program's roundings to bfloat16 on the way count: a program that leaves them out, or rounds other values in their place, can miss the bound.
Values may be sent and summed in bfloat16 or wider, within the bound.
A program may use at most 64 MiB of HBM per device.

```python
import jax
import jax.numpy as jnp
from jax import lax

MODEL_WIDTH = 2048
HEAD_SIZE = 64
QUERY_HEADS = 16
KEY_VALUE_HEADS = 4
WINDOW = 128
POOL_GROUPS = 4
POOL_CH = 256
LEN = 2048
SEQS = 4


def draw_query_weight(key, part):
    base = jax.random.normal(jax.random.fold_in(key, 11), (MODEL_WIDTH, QUERY_HEADS * HEAD_SIZE), jnp.float32)
    base = jnp.clip(base, -6.0, 6.0) * MODEL_WIDTH ** (-0.5)
    return jnp.clip(base, -20.0, 20.0).astype(jnp.bfloat16)


def levels(rng, shape, shards, least, high):
    def one(axis_at, parts):
        heights = jax.random.uniform(jax.random.fold_in(jax.random.fold_in(rng, 6), axis_at), (parts,), jnp.float32, least / len(shards), high / len(shards))
        return jnp.repeat(jnp.exp(heights), shape[axis_at] // parts).reshape((-1,) + (1,) * (len(shape) - axis_at - 1))

    level = one(*shards[0])
    for cut in shards[1:]:
        level = level * one(*cut)
    return level


def bell_draw(rng, extent, deviation, reach, cuts=(), kind=jnp.bfloat16):
    values = deviation * jax.random.normal(rng, extent, jnp.float32)
    if cuts:
        values = values * levels(rng, extent, cuts, -0.22, 0.18)
    return jnp.clip(values, -reach, reach).astype(kind)


def setup_inputs(seed: int = 0) -> dict:
    seeds = jax.random.split(jax.random.key(seed), 12)
    return {
        "tokens": bell_draw(seeds[0], (SEQS, LEN, MODEL_WIDTH), 1.0, 6.0, ((0, 4), (1, 8))),
        "norm_gain": jnp.clip(1.0 + 0.18 * jax.random.normal(seeds[1], (MODEL_WIDTH,), jnp.float32), 0.1, 1.9),
        "query_weight": draw_query_weight(jax.random.fold_in(seeds[11], 71), 0),
        "key_matrix": bell_draw(seeds[3], (MODEL_WIDTH, KEY_VALUE_HEADS * HEAD_SIZE), MODEL_WIDTH ** -0.5, 0.125, ((0, 4), (1, 2))),
        "value_matrix": bell_draw(seeds[4], (MODEL_WIDTH, KEY_VALUE_HEADS * HEAD_SIZE), MODEL_WIDTH ** -0.5, 0.125, ((0, 4), (1, 2))),
        "pool_in_weight": bell_draw(seeds[5], (MODEL_WIDTH, POOL_GROUPS * POOL_CH), MODEL_WIDTH ** -0.5, 0.125, ((0, 4), (1, 2))),
        "head_sink_logit": jnp.clip(jax.random.uniform(seeds[6], (QUERY_HEADS,), jnp.float32, 2.0, 6.0), 2.0, 6.0),
        "pool_mix": bell_draw(seeds[7], (POOL_GROUPS, POOL_CH, POOL_CH), POOL_CH ** -0.5, 0.375),
        "pool_gain": jnp.clip(1.0 + 0.18 * jax.random.normal(seeds[8], (POOL_GROUPS * POOL_CH,), jnp.float32), 0.1, 1.9),
        "attn_out_weight": bell_draw(seeds[9], (QUERY_HEADS * HEAD_SIZE, MODEL_WIDTH), (QUERY_HEADS * HEAD_SIZE // 32) ** -0.5, 1.0, ((0, 2), (1, 4))),
        "pool_out_weight": bell_draw(seeds[10], (POOL_GROUPS * POOL_CH, MODEL_WIDTH), (QUERY_HEADS * HEAD_SIZE + POOL_GROUPS * POOL_CH) ** -0.5, 0.125, ((0, 2), (1, 4))),
    }


EPSILON = 1e-06
POOL_SPANS = (2, 4, 8, 16)

def windowed_attend(query_rows, key_rows, value_rows, sinks, kv_heads, group):
    rows = query_rows.shape[0]
    blocks = rows // WINDOW
    width = key_rows.shape[1]
    ext_keys = jnp.concatenate([jnp.zeros((WINDOW, width), key_rows.dtype), key_rows], 0)
    ext_values = jnp.concatenate([jnp.zeros((WINDOW, width), value_rows.dtype), value_rows], 0)

    def banded(table):
        return jnp.concatenate([table[:rows].reshape(blocks, WINDOW, width), table[WINDOW:].reshape(blocks, WINDOW, width)], axis=1)
    band_keys = banded(ext_keys).reshape(blocks, 2 * WINDOW, kv_heads, HEAD_SIZE).astype(jnp.float32)
    band_values = banded(ext_values).reshape(blocks, 2 * WINDOW, kv_heads, HEAD_SIZE).astype(jnp.float32)
    query_blocks = query_rows.reshape(blocks, WINDOW, kv_heads, group, HEAD_SIZE).astype(jnp.float32)
    scores = jnp.einsum('bqkgd,bskd->bkgqs', query_blocks, band_keys) * HEAD_SIZE ** (-0.5)
    query_pos = jnp.arange(rows).reshape(blocks, WINDOW, 1)
    key_pos = jnp.arange(blocks).reshape(blocks, 1, 1) * WINDOW - WINDOW + jnp.arange(2 * WINDOW).reshape(1, 1, 2 * WINDOW)
    offset = query_pos - key_pos
    allowed = (offset >= 0) & (offset < WINDOW) & (key_pos >= 0)
    scores = jnp.where(allowed[:, None, None], scores, -jnp.inf)
    sink_grid = sinks.astype(jnp.float32).reshape(1, kv_heads, group, 1, 1)
    top = jnp.maximum(lax.optimization_barrier(jnp.max(scores, axis=-1, keepdims=True)), sink_grid)
    weights = jnp.exp(scores - top)
    total = lax.optimization_barrier(jnp.sum(weights, axis=-1, keepdims=True)) + jnp.exp(sink_grid - top)
    probs = (weights / total).astype(jnp.bfloat16).astype(jnp.float32)
    mixed = jnp.einsum('bkgqs,bskd->bqkgd', probs, band_values).astype(jnp.bfloat16)
    row_log_weight_sum = (top + jnp.log(total))[..., 0]
    return (mixed.reshape(rows, kv_heads * group * HEAD_SIZE), row_log_weight_sum.transpose(1, 2, 0, 3).reshape(kv_heads * group, rows))

def pool_branch(pool_input, pool_mix, pool_gain):
    rows = pool_input.shape[0]
    pool_reach = max(POOL_SPANS)
    padded = jnp.concatenate([jnp.zeros((pool_reach, pool_input.shape[1]), jnp.float32), pool_input.astype(jnp.float32)], 0)
    position = jnp.arange(rows).reshape(rows, 1)
    pieces = []
    for index, span in enumerate(POOL_SPANS):
        columns = padded[:, index * POOL_CH:(index + 1) * POOL_CH]
        trailing = jnp.zeros((rows, POOL_CH), jnp.float32)
        for lag in range(span):
            trailing = trailing + columns[pool_reach - lag:pool_reach - lag + rows]
        count = jnp.minimum(position + 1, span).astype(jnp.float32)
        pieces.append(trailing / count - columns[pool_reach:])
    centred = jnp.concatenate(pieces, axis=1).astype(jnp.bfloat16)
    grouped = centred.reshape(rows, POOL_GROUPS, POOL_CH).astype(jnp.float32)
    product = jnp.einsum('rgc,gcd->rgd', grouped, pool_mix.astype(jnp.float32)).reshape(rows, POOL_GROUPS * POOL_CH)
    return (product * pool_gain).astype(jnp.bfloat16)

def reference(tokens, norm_gain, query_weight, key_matrix, value_matrix, pool_in_weight, head_sink_logit, pool_mix, pool_gain, attn_out_weight, pool_out_weight):

    def one_sequence(sequence):
        values_f = sequence.astype(jnp.float32)
        scale = lax.rsqrt(lax.optimization_barrier(jnp.mean(values_f * values_f, axis=-1, keepdims=True)) + EPSILON)
        normed = (values_f * scale * norm_gain).astype(jnp.bfloat16)
        query_rows = jnp.dot(normed, query_weight, preferred_element_type=jnp.float32).astype(jnp.bfloat16)
        key_rows = jnp.dot(normed, key_matrix, preferred_element_type=jnp.float32).astype(jnp.bfloat16)
        value_rows = jnp.dot(normed, value_matrix, preferred_element_type=jnp.float32).astype(jnp.bfloat16)
        pool_input = jnp.dot(normed, pool_in_weight, preferred_element_type=jnp.float32).astype(jnp.bfloat16)
        attention_mixer, row_log_weight_sum = windowed_attend(query_rows, key_rows, value_rows, head_sink_logit, KEY_VALUE_HEADS, QUERY_HEADS // KEY_VALUE_HEADS)
        pool_out = pool_branch(pool_input, pool_mix, pool_gain)
        result = jnp.dot(attention_mixer, attn_out_weight, preferred_element_type=jnp.float32) + jnp.dot(pool_out, pool_out_weight, preferred_element_type=jnp.float32)
        return (result.astype(jnp.bfloat16), row_log_weight_sum)
    mixed, row_log_weight_sum = lax.map(one_sequence, tokens)
    return (mixed, row_log_weight_sum)
```

```python
import functools

import jax
import jax.numpy as jnp
from jax import lax
from jax.experimental import pallas as pl
from jax.experimental.pallas import tpu as pltpu
from jax.sharding import PartitionSpec as P

HEAD_SIZE = 64
WINDOW = 128
POOL_CH = 256


EPSILON = 1e-06
POOL_SPANS = (2, 4, 8, 16)


def passed_along(shard, axis, by):
    size = lax.axis_size(axis)
    pairs = [(i, i + by) for i in range(size) if 0 <= i + by < size]
    return lax.ppermute(shard, axis, pairs)


def windowed_attend(
    query_rows, key_rows, value_rows, key_tail, value_tail, sinks, kv_heads, group, first_pos
):
    rows = query_rows.shape[0]
    blocks = rows // WINDOW
    width = key_rows.shape[1]
    ext_keys = jnp.concatenate([key_tail, key_rows], 0)
    ext_values = jnp.concatenate([value_tail, value_rows], 0)

    def banded(table):
        return jnp.concatenate(
            [
                table[:rows].reshape(blocks, WINDOW, width),
                table[WINDOW:].reshape(blocks, WINDOW, width),
            ],
            axis=1,
        )

    band_keys = banded(ext_keys).reshape(blocks, 2 * WINDOW, kv_heads, HEAD_SIZE)
    band_values = banded(ext_values).reshape(blocks, 2 * WINDOW, kv_heads, HEAD_SIZE)
    query_blocks = query_rows.reshape(blocks, WINDOW, kv_heads, group, HEAD_SIZE)
    scores = jnp.einsum(
        "bqkgd,bskd->bkgqs", query_blocks, band_keys, preferred_element_type=jnp.float32
    ) * HEAD_SIZE ** (-0.5)
    query_pos = first_pos + jnp.arange(rows).reshape(blocks, WINDOW, 1)
    key_pos = (
        first_pos
        - WINDOW
        + jnp.arange(blocks).reshape(blocks, 1, 1) * WINDOW
        + jnp.arange(2 * WINDOW).reshape(1, 1, 2 * WINDOW)
    )
    offset = query_pos - key_pos
    allowed = (offset >= 0) & (offset < WINDOW) & (key_pos >= 0)
    scores = jnp.where(allowed[:, None, None], scores, -jnp.inf)
    sink_grid = sinks.reshape(1, kv_heads, group, 1, 1)
    top = jnp.maximum(jnp.max(scores, axis=-1, keepdims=True), sink_grid)
    weights = jnp.exp(scores - top)
    total = jnp.sum(weights, axis=-1, keepdims=True) + jnp.exp(sink_grid - top)
    probs = (weights / total).astype(jnp.bfloat16)
    mixed = jnp.einsum(
        "bkgqs,bskd->bqkgd", probs, band_values, preferred_element_type=jnp.float32
    ).astype(jnp.bfloat16)
    row_log_weight_sum = (top + jnp.log(total))[..., 0]
    return (
        mixed.reshape(rows, kv_heads * group * HEAD_SIZE),
        row_log_weight_sum.transpose(1, 2, 0, 3).reshape(kv_heads * group, rows),
    )


def pool_branch(pool_rows, pool_tail, mixing, scales, group_start, first_pos):
    rows = pool_rows.shape[0]
    columns = pool_rows.shape[1]
    pool_reach = max(POOL_SPANS)
    extended = jnp.concatenate([pool_tail, pool_rows], 0).astype(jnp.float32)
    group_index = group_start + jnp.arange(columns) // POOL_CH
    span_table = jnp.array(POOL_SPANS, jnp.int32)
    matches = group_index[:, None] == jnp.arange(len(POOL_SPANS))[None, :]
    span_of_col = jnp.sum(jnp.where(matches, span_table[None, :], 0), axis=1)
    trailing = jnp.zeros((rows, columns), jnp.float32)
    for lag in range(pool_reach):
        trailing = trailing + jnp.where(
            lag < span_of_col[None, :], extended[pool_reach - lag : pool_reach - lag + rows], 0.0
        )
    position = first_pos + jnp.arange(rows)
    count = jnp.minimum(position[:, None] + 1, span_of_col[None, :]).astype(jnp.float32)
    centred = (trailing / count - extended[pool_reach:]).astype(jnp.bfloat16)
    grouped = centred.reshape(rows, columns // POOL_CH, POOL_CH)
    product = jnp.einsum(
        "rgc,gcd->rgd", grouped, mixing, preferred_element_type=jnp.float32
    ).reshape(rows, columns)
    return (product * scales).astype(jnp.bfloat16)


def local(
    tokens,
    norm_gain,
    query_weight,
    key_matrix,
    value_matrix,
    pool_in_weight,
    head_sink_logit,
    pool_mix,
    pool_gain,
    attn_out_weight,
    pool_out_weight,
):
    tp_index = lax.axis_index("tp")
    sp_index = lax.axis_index("sp")
    q_cols = query_weight.shape[1]
    kv_cols = key_matrix.shape[1]
    pool_cols = pool_in_weight.shape[1]
    q_heads = q_cols // HEAD_SIZE
    kv_heads = kv_cols // HEAD_SIZE
    groups_dev = pool_cols // POOL_CH
    full_query, full_key, full_value, full_pool = (
        lax.all_gather(query_weight, "sp", axis=0, tiled=True),
        lax.all_gather(key_matrix, "sp", axis=0, tiled=True),
        lax.all_gather(value_matrix, "sp", axis=0, tiled=True),
        lax.all_gather(pool_in_weight, "sp", axis=0, tiled=True),
    )
    values_f = lax.all_gather(tokens[0], "tp", axis=0, tiled=True).astype(jnp.float32)
    scale = lax.rsqrt(jnp.mean(values_f * values_f, axis=-1, keepdims=True) + EPSILON)
    normed = (values_f * scale * norm_gain).astype(jnp.bfloat16)
    outputs = [
        jnp.dot(normed, weight, preferred_element_type=jnp.float32).astype(jnp.bfloat16)
        for weight in (full_query, full_key, full_value, full_pool)
    ]
    projected = jnp.concatenate(outputs, axis=1)
    rows = projected.shape[0]
    first_pos = sp_index * rows
    query_rows = projected[:, :q_cols]
    key_rows = projected[:, q_cols : q_cols + kv_cols]
    value_rows = projected[:, q_cols + kv_cols : q_cols + 2 * kv_cols]
    pool_rows = projected[:, q_cols + 2 * kv_cols :]
    pool_reach = max(POOL_SPANS)
    sinks = lax.dynamic_slice_in_dim(head_sink_logit, tp_index * q_heads, q_heads, 0)
    mixing = lax.dynamic_slice_in_dim(pool_mix, tp_index * groups_dev, groups_dev, 0)
    scales = lax.dynamic_slice_in_dim(pool_gain, tp_index * pool_cols, pool_cols, 0)
    key_tail, value_tail, pool_tail = passed_along(
        (key_rows[rows - WINDOW :], value_rows[rows - WINDOW :], pool_rows[rows - pool_reach :]),
        "sp",
        1,
    )
    attn_part, log_part = windowed_attend(
        query_rows,
        key_rows,
        value_rows,
        key_tail,
        value_tail,
        sinks,
        kv_heads,
        q_heads // kv_heads,
        first_pos,
    )
    pool_part = pool_branch(pool_rows, pool_tail, mixing, scales, tp_index * groups_dev, first_pos)
    half_attn, half_pool = (
        lax.all_gather(attn_out_weight, "sp", axis=1, tiled=True),
        lax.all_gather(pool_out_weight, "sp", axis=1, tiled=True),
    )
    result = lax.psum_scatter(
        jnp.dot(attn_part, half_attn, preferred_element_type=jnp.float32)
        + jnp.dot(pool_part, half_pool, preferred_element_type=jnp.float32),
        "tp",
        scatter_dimension=0,
        tiled=True,
    ).astype(jnp.bfloat16)
    return (result[None], log_part[None])


LANES = 128
TILE = 16
MESH_ID = pl.DeviceIdType.MESH


def nearest(n, step, me):
    tables = [sorted((j for j in range(n) if j != z), key=lambda j: (abs(j - z), j)) for z in range(n)]
    shard = jnp.int32(tables[0][step])
    for z in range(1, n):
        shard = jnp.where(me == z, tables[z][step], shard)
    return shard


def layer_kernel(
    n,
    sinks,
    tokens,
    gain,
    wq,
    wk,
    wv,
    wp,
    mix,
    pool_gain,
    wao,
    wpo,
    out,
    log_out,
    held,
    tok,
    normed,
    proj,
    kv,
    pool_ext,
    mixed,
    mix_own,
    mine,
    sent,
    got,
    z_send,
    x_send,
    y_send,
    z_recv,
    x_recv,
    y_recv,
    load_sem,
    tok_sem,
    halo_send,
    halo_recv,
    sum_send,
    sum_recv,
):
    me = lax.axis_index("sp")
    f = lax.axis_index("fs")
    c = lax.axis_index("tp")
    f32 = jnp.float32
    half = tokens.shape[0]
    rows = 2 * half
    depth = wq.shape[0]
    n_in = (wq.shape[1] + wk.shape[1] + wv.shape[1] + wp.shape[1]) // LANES
    out_tiles = wao.shape[1] // LANES
    n_blocks = n_in + 2 * out_tiles
    steps = n_blocks // 3
    sources = [wk, wv] + [wq.at[:, pl.ds(i * LANES, LANES)] for i in range(wq.shape[1] // LANES)]
    sources += [wp.at[:, pl.ds(i * LANES, LANES)] for i in range(wp.shape[1] // LANES)]
    for i in range(out_tiles):
        sources += [w.at[:, pl.ds(i * LANES, LANES)] for w in (wao, wpo)]
    z_part = lax.rem(f, 3)
    beside = f + 1 - 2 * lax.rem(f, 2)
    across = lax.rem(f + 2, 4)
    x_part = lax.rem(beside, 3)
    y_part = 3 - z_part - x_part
    relays = (f == 0) | (f == 3)
    y_out = jnp.where(relays, x_part, z_part)
    up, down = me + 1, me - 1
    has_up, has_down = me < n - 1, me > 0

    def load(i):
        return pltpu.make_async_copy(sources[i], held.at[me, i], load_sem.at[i])

    for i in range(n_blocks):
        load(i).start()
    own_rows = pl.ds(pl.multiple_of(c * half, half), half)
    tok_load = pltpu.make_async_copy(tokens, tok.at[own_rows], tok_sem.at[2])
    tok_load.start()
    groups = mix_own.shape[0]
    mix_load = pltpu.make_async_copy(mix.at[pl.ds(c * groups, groups)], mix_own, tok_sem.at[3])
    mix_load.start()

    barrier = pltpu.get_barrier_semaphore()
    pl.semaphore_signal(barrier, inc=1, device_id={"tp": 1 - c}, device_id_type=MESH_ID)
    pl.semaphore_signal(barrier, inc=1, device_id={"fs": beside}, device_id_type=MESH_ID)
    pl.semaphore_signal(barrier, inc=1, device_id={"fs": across}, device_id_type=MESH_ID)

    @pl.when(has_up)
    def _():
        pl.semaphore_signal(barrier, inc=1, device_id={"sp": up}, device_id_type=MESH_ID)

    @pl.when(has_down)
    def _():
        pl.semaphore_signal(barrier, inc=1, device_id={"sp": down}, device_id_type=MESH_ID)

    pl.semaphore_wait(barrier, 3 + has_up.astype(jnp.int32) + has_down.astype(jnp.int32))

    tok_send = pltpu.make_async_remote_copy(
        tokens, tok.at[own_rows], tok_sem.at[0], tok_sem.at[1],
        device_id={"tp": 1 - c}, device_id_type=MESH_ID,
    )
    tok_send.start()

    def hop(s, j, part, send, recv, to):
        block = held.at[j, 3 * s + part]
        return pltpu.make_async_remote_copy(
            block, block, send, recv.at[s, j], device_id=to, device_id_type=MESH_ID
        )

    def z_hop(s, j, way):
        to = jnp.where(way == 0, up, down)
        return hop(s, j, z_part, z_send.at[way, s, j], z_recv, {"sp": to})

    def x_hop(s, j):
        return hop(s, j, z_part, x_send.at[s, j], x_recv, {"fs": beside})

    def y_hop(s, j):
        return hop(s, j, y_out, y_send.at[s, j], y_recv, {"fs": across})

    def onward(j):
        return jnp.where(j < me, 0, 1), ((j < me) & has_up) | ((j > me) & has_down)

    def own_send(s, finish=False):
        @pl.when(has_up)
        def _():
            cp = z_hop(s, me, 0)
            cp.wait_send() if finish else cp.start()

        @pl.when(has_down)
        def _():
            cp = z_hop(s, me, 1)
            cp.wait_send() if finish else cp.start()

    slots = [(s, k) for s in range(steps) for k in range(n - 1)]
    shard = [nearest(n, k, me) for k in range(n - 1)]

    def z_step(t):
        s, k = slots[t]
        j = shard[k]
        if k == 0 and s + 1 < steps:
            own_send(s + 1)
        z_hop(s, j, 0).wait_recv()
        way, more = onward(j)

        @pl.when(more)
        def _():
            z_hop(s, j, way).start()

        x_hop(s, j).start()

    def x_step(t):
        s, k = slots[t]
        hop(s, shard[k], x_part, x_send.at[s, shard[k]], x_recv, {"fs": beside}).wait_recv()
        y_hop(s, shard[k]).start()

    def y_step(t):
        s, k = slots[t]
        hop(s, shard[k], y_part, y_send.at[s, shard[k]], y_recv, {"fs": across}).wait_recv()

    for i in range(n_blocks):
        load(i).wait()
        if i % 3 == 2 and i // 3 == 0:
            own_send(0)

    def norm_rows(r, size):
        v = tok[pl.ds(r, size), :].astype(f32)
        scale = lax.rsqrt(jnp.mean(v * v, axis=-1, keepdims=True) + EPSILON)
        normed[pl.ds(r, size), :] = (v * scale * gain[...]).astype(jnp.bfloat16)

    def norm_all():
        tok_load.wait()
        tok_send.wait()
        mix_load.wait()
        chunk = 32

        @pl.loop(0, rows // chunk)
        def _(i):
            norm_rows(pl.multiple_of(i * chunk, chunk), chunk)

    def project(pair):
        acc = None
        for j in range(n):
            w = jnp.concatenate([held[j, 2 * pair], held[j, 2 * pair + 1]], axis=1)
            term = jnp.dot(normed[:, j * depth : (j + 1) * depth], w, preferred_element_type=f32)
            acc = term if acc is None else acc + term
        return acc.astype(jnp.bfloat16)

    def halo_kv():
        return pltpu.make_async_remote_copy(
            kv.at[pl.ds(rows, WINDOW)], kv.at[pl.ds(0, WINDOW)], halo_send.at[0], halo_recv.at[0],
            device_id={"sp": up}, device_id_type=MESH_ID,
        )

    def halo_pool(g):
        return pltpu.make_async_remote_copy(
            pool_ext.at[g, pl.ds(rows, TILE)], pool_ext.at[g, pl.ds(0, TILE)],
            halo_send.at[1 + g], halo_recv.at[1 + g],
            device_id={"sp": up}, device_id_type=MESH_ID,
        )

    def first_zero(store):
        @pl.when(me == 0)
        def _():
            store()

    def project_kv():
        kv[pl.ds(WINDOW, rows), :] = project(0)

        @pl.when(has_up)
        def _():
            halo_kv().start()

        def zero():
            kv[pl.ds(0, WINDOW), :] = jnp.zeros((WINDOW, kv.shape[1]), kv.dtype)

        first_zero(zero)

    def project_q(g):
        proj[g] = project(1 + g)

    kv_cols = wk.shape[1]
    kv_heads = kv_cols // HEAD_SIZE
    group = wq.shape[1] // HEAD_SIZE // kv_heads

    def project_pool(g):
        pool_ext[g, pl.ds(TILE, rows), :] = project(1 + kv_heads + g)

        @pl.when(has_up)
        def _():
            halo_pool(g).start()

        def zero():
            pool_ext[g, pl.ds(0, TILE), :] = jnp.zeros((TILE, POOL_CH), pool_ext.dtype)

        first_zero(zero)

    def kv_arrived():
        @pl.when(has_down)
        def _():
            halo_kv().wait_recv()

    def attend(b):
        base = b * WINDOW
        lane = lax.broadcasted_iota(jnp.int32, (WINDOW, LANES), 1)
        logs = jnp.zeros((WINDOW, LANES), f32)
        i_pos = lax.broadcasted_iota(jnp.int32, (WINDOW, 2 * WINDOW), 0)
        k_pos = lax.broadcasted_iota(jnp.int32, (WINDOW, 2 * WINDOW), 1)
        allowed = (k_pos > i_pos) & (k_pos <= i_pos + WINDOW)
        allowed = allowed & (k_pos + (me * rows + base - WINDOW) >= 0)
        for g in range(kv_heads):
            band = kv[pl.ds(base, 2 * WINDOW), :]
            keys = band[:, g * HEAD_SIZE : (g + 1) * HEAD_SIZE]
            vals = band[:, kv_cols + g * HEAD_SIZE : kv_cols + (g + 1) * HEAD_SIZE]
            q = proj[g, pl.ds(base, WINDOW), :]
            q = jnp.concatenate([q[:, h * HEAD_SIZE : (h + 1) * HEAD_SIZE] for h in range(group)], axis=0)
            scores = lax.dot_general(q, keys, (((1,), (1,)), ((), ())), preferred_element_type=f32)
            probs = []
            for h in range(group):
                head = g * group + h
                sink = sinks[c * kv_heads * group + head]
                sc = jnp.where(allowed, scores[h * WINDOW : (h + 1) * WINDOW] * HEAD_SIZE**-0.5, -jnp.inf)
                top = jnp.maximum(jnp.max(sc, axis=-1, keepdims=True), sink)
                w = jnp.exp(sc - top)
                total = jnp.sum(w, axis=-1, keepdims=True) + jnp.exp(sink - top)
                probs.append((w * (1.0 / total)).astype(jnp.bfloat16))
                logs = jnp.where(lane == head, top + jnp.log(total), logs)
            res = jnp.dot(jnp.concatenate(probs, axis=0), vals, preferred_element_type=f32)
            res = jnp.concatenate([res[h * WINDOW : (h + 1) * WINDOW] for h in range(group)], axis=1)
            mixed[g, pl.ds(base, WINDOW), :] = res.astype(jnp.bfloat16)
        log_out[:, pl.ds(base, WINDOW)] = jnp.transpose(logs)[: kv_heads * group]

    def pool(g):
        @pl.when(has_down)
        def _():
            halo_pool(g).wait_recv()

        index = c * groups + g
        run = pool_ext[g].astype(f32)
        own = run[TILE:]
        trailing = jnp.zeros_like(run)
        span_here = jnp.int32(0)
        reach = 1
        for at, span in enumerate(POOL_SPANS):
            while reach < span:
                run = run + pltpu.roll(run, reach, 0)
                reach *= 2
            trailing = jnp.where(index == at, run, trailing)
            span_here = jnp.where(index == at, span, span_here)
        pos = me * rows + lax.broadcasted_iota(jnp.int32, (rows, 1), 0)
        count = jnp.minimum(pos + 1, span_here).astype(f32)
        centred = (trailing[TILE:] / count - own).astype(jnp.bfloat16)
        product = jnp.dot(centred, mix_own[g], preferred_element_type=f32)
        mixed[kv_heads + g] = (product * pool_gain[index]).astype(jnp.bfloat16)

    n_pairs = out_tiles // 2

    def sum_hop(slot):
        return pltpu.make_async_remote_copy(
            sent.at[slot], got.at[slot], sum_send.at[slot], sum_recv.at[slot],
            device_id={"tp": 1 - c}, device_id_type=MESH_ID,
        )

    def out_project(j, pair):
        slot = j * n_pairs + pair
        acc = None
        for side in range(2):
            first = n_in + 4 * pair + side
            w = jnp.concatenate([held[j, first], held[j, first + 2]], axis=1)
            parts = mixed.shape[0] // 2
            a = jnp.concatenate([mixed[side * parts + i] for i in range(parts)], axis=1)
            term = jnp.dot(a, w, preferred_element_type=f32)
            acc = term if acc is None else acc + term
        low, high = acc[:half], acc[half:]
        mine[slot] = jnp.where(c == 0, low, high)
        sent[slot] = jnp.where(c == 0, high, low)
        sum_hop(slot).start()

    def finish(j, pair):
        slot = j * n_pairs + pair
        sum_hop(slot).wait()
        wide = 2 * LANES
        cols = pl.ds(pl.multiple_of(slot * wide, wide), wide)
        out[:, cols] = (mine[slot] + got[slot]).astype(jnp.bfloat16)

    tasks = {}

    def ready(block):
        return (block // 3) * (n - 1) + n - 2

    def at(t, task, *args):
        tasks.setdefault(min(t, len(slots) - 1), []).append((task, args))

    at(-1, norm_all)
    at(ready(1), project_kv)
    for g in range(kv_heads):
        at(ready(2 * g + 3), project_q, g)
    last = ready(2 * kv_heads + 1) + 1
    at(last, kv_arrived)
    for b in range(rows // WINDOW):
        at(last + b // 2, attend, b)
    for g in range(groups):
        at(ready(2 * (1 + kv_heads + g) + 1), project_pool, g)
    for g in range(groups):
        at(ready(2 * (kv_heads + groups) + 1) + (g + 1) // 2, pool, g)
    base_slot = ready(n_in - 1) + 1
    for pair in range(n_pairs):
        at(base_slot, out_project, me, pair)
    for k in range(n - 1):
        for pair in range(n_pairs):
            when = ((n_in + 4 * pair + 3) // 3) * (n - 1) + k
            at(max(when, base_slot), out_project, shard[k], pair)

    total_slots = len(slots)
    for t in range(-1, total_slots + 2):
        if 0 <= t < total_slots:
            z_step(t)
        if 0 <= t - 1 < total_slots:
            x_step(t - 1)
        if 0 <= t - 2 < total_slots:
            y_step(t - 2)
        here = t if t < 0 else t - 2
        if t in (0, 1):
            continue
        for task, args in tasks.pop(here, ()):
            task(*args)
    for j in [me] + shard:
        for pair in range(n_pairs):
            finish(j, pair)

    for s in range(steps):
        own_send(s, finish=True)
    for s, k in slots:
        way, more = onward(shard[k])

        @pl.when(more)
        def _():
            z_hop(s, shard[k], way).wait_send()

        x_hop(s, shard[k]).wait_send()
        y_hop(s, shard[k]).wait_send()

    @pl.when(has_up)
    def _():
        halo_kv().wait_send()
        for g in range(groups):
            halo_pool(g).wait_send()


def fused_local(
    n,
    tokens,
    norm_gain,
    query_weight,
    key_matrix,
    value_matrix,
    pool_in_weight,
    head_sink_logit,
    pool_mix,
    pool_gain,
    attn_out_weight,
    pool_out_weight,
):
    _, half, width = tokens.shape
    rows = 2 * half
    depth, q_cols = query_weight.shape
    kv_cols = key_matrix.shape[1]
    pool_cols = pool_in_weight.shape[1]
    heads = q_cols // HEAD_SIZE
    kv_heads = kv_cols // HEAD_SIZE
    groups = pool_cols // POOL_CH
    n_in = (q_cols + 2 * kv_cols + pool_cols) // LANES
    n_blocks = n_in + 2 * attn_out_weight.shape[1] // LANES
    steps = n_blocks // 3
    pieces = n * attn_out_weight.shape[1] // (2 * LANES)
    bf16, f32 = jnp.bfloat16, jnp.float32
    dma = pltpu.SemaphoreType.DMA
    hbm = pl.BlockSpec(memory_space=pl.ANY)
    vmem = pl.BlockSpec(memory_space=pltpu.VMEM)
    smem = pl.BlockSpec(memory_space=pltpu.SMEM)
    mixed, logs = pl.pallas_call(
        functools.partial(layer_kernel, n),
        out_shape=(
            jax.ShapeDtypeStruct((half, width), bf16),
            jax.ShapeDtypeStruct((heads, rows), f32),
        ),
        in_specs=[smem, hbm, vmem, hbm, hbm, hbm, hbm, hbm, vmem, hbm, hbm],
        out_specs=(vmem, vmem),
        scratch_shapes=[
            pltpu.VMEM((n, n_blocks, depth, LANES), bf16),
            pltpu.VMEM((rows, width), bf16),
            pltpu.VMEM((rows, width), bf16),
            pltpu.VMEM((kv_heads, rows, 2 * LANES), bf16),
            pltpu.VMEM((WINDOW + rows, 2 * kv_cols), bf16),
            pltpu.VMEM((groups, TILE + rows, POOL_CH), bf16),
            pltpu.VMEM((kv_heads + groups, rows, 2 * LANES), bf16),
            pltpu.VMEM((groups, POOL_CH, POOL_CH), bf16),
            pltpu.VMEM((pieces, half, 2 * LANES), f32),
            pltpu.VMEM((pieces, half, 2 * LANES), f32),
            pltpu.VMEM((pieces, half, 2 * LANES), f32),
            dma((2, steps, n)),
            dma((steps, n)),
            dma((steps, n)),
            dma((steps, n)),
            dma((steps, n)),
            dma((steps, n)),
            dma((n_blocks,)),
            dma((4,)),
            dma((1 + groups,)),
            dma((1 + groups,)),
            dma((pieces,)),
            dma((pieces,)),
        ],
        compiler_params=pltpu.CompilerParams(
            collective_id=0, has_side_effects=True, vmem_limit_bytes=60 * 1024 * 1024
        ),
    )(
        head_sink_logit,
        tokens[0],
        norm_gain.reshape(1, width),
        query_weight,
        key_matrix,
        value_matrix,
        pool_in_weight,
        pool_mix,
        pool_gain.reshape(-1, 1, POOL_CH),
        attn_out_weight,
        pool_out_weight,
    )
    return mixed[None], logs[None]


def fits(mesh, tokens, query_weight, key_matrix, pool_in_weight, attn_out_weight):
    n, f, c = mesh.shape["sp"], mesh.shape["fs"], mesh.shape["tp"]
    depth = query_weight.shape[0] // n
    rows = tokens.shape[1] // n
    q_cols, kv_cols, pool_cols = (w.shape[1] // c for w in (query_weight, key_matrix, pool_in_weight))
    tiles = attn_out_weight.shape[1] // n // LANES
    blocks = (q_cols + 2 * kv_cols + pool_cols) // LANES + 2 * tiles
    return (
        2 <= n <= 4
        and f == 4
        and c == 2
        and tokens.shape[0] == f
        and rows % WINDOW == 0
        and kv_cols == LANES
        and q_cols == 2 * LANES * (kv_cols // HEAD_SIZE)
        and pool_cols == q_cols
        and POOL_CH == 2 * LANES
        and attn_out_weight.shape[1] % (n * 2 * LANES) == 0
        and attn_out_weight.shape[0] // c == depth
        and depth % LANES == 0
        and blocks % 3 == 0
    )


def solution(mesh):
    in_specs = (
        P("fs", ("sp", "tp"), None),
        P(),
        P("sp", "tp"),
        P("sp", "tp"),
        P("sp", "tp"),
        P("sp", "tp"),
        P(),
        P(),
        P(),
        P("tp", "sp"),
        P("tp", "sp"),
    )
    out_specs = (P("fs", ("sp", "tp"), None), P("fs", "tp", "sp"))

    def step(*args):
        fused = fits(mesh, args[0], args[2], args[3], args[5], args[9])
        body = functools.partial(fused_local, mesh.shape["sp"]) if fused else local
        mapped = jax.shard_map(body, mesh=mesh, in_specs=in_specs, out_specs=out_specs, check_vma=False)
        return mapped(*args)

    return step
```

```python
import functools

import jax
import jax.numpy as jnp
from jax import lax
from jax.experimental import pallas as pl
from jax.experimental.pallas import tpu as pltpu
from jax.sharding import PartitionSpec as P

HEAD_SIZE = 64
WINDOW = 128
POOL_CH = 256


EPSILON = 1e-06
POOL_SPANS = (2, 4, 8, 16)


def passed_along(shard, axis, by):
    size = lax.axis_size(axis)
    pairs = [(i, i + by) for i in range(size) if 0 <= i + by < size]
    return lax.ppermute(shard, axis, pairs)


def windowed_attend(
    query_rows, key_rows, value_rows, key_tail, value_tail, sinks, kv_heads, group, first_pos
):
    rows = query_rows.shape[0]
    blocks = rows // WINDOW
    width = key_rows.shape[1]
    ext_keys = jnp.concatenate([key_tail, key_rows], 0)
    ext_values = jnp.concatenate([value_tail, value_rows], 0)

    def banded(table):
        return jnp.concatenate(
            [
                table[:rows].reshape(blocks, WINDOW, width),
                table[WINDOW:].reshape(blocks, WINDOW, width),
            ],
            axis=1,
        )

    band_keys = banded(ext_keys).reshape(blocks, 2 * WINDOW, kv_heads, HEAD_SIZE)
    band_values = banded(ext_values).reshape(blocks, 2 * WINDOW, kv_heads, HEAD_SIZE)
    query_blocks = query_rows.reshape(blocks, WINDOW, kv_heads, group, HEAD_SIZE)
    scores = jnp.einsum(
        "bqkgd,bskd->bkgqs", query_blocks, band_keys, preferred_element_type=jnp.float32
    ) * HEAD_SIZE ** (-0.5)
    query_pos = first_pos + jnp.arange(rows).reshape(blocks, WINDOW, 1)
    key_pos = (
        first_pos
        - WINDOW
        + jnp.arange(blocks).reshape(blocks, 1, 1) * WINDOW
        + jnp.arange(2 * WINDOW).reshape(1, 1, 2 * WINDOW)
    )
    offset = query_pos - key_pos
    allowed = (offset >= 0) & (offset < WINDOW) & (key_pos >= 0)
    scores = jnp.where(allowed[:, None, None], scores, -jnp.inf)
    sink_grid = sinks.reshape(1, kv_heads, group, 1, 1)
    top = jnp.maximum(jnp.max(scores, axis=-1, keepdims=True), sink_grid)
    weights = jnp.exp(scores - top)
    total = jnp.sum(weights, axis=-1, keepdims=True) + jnp.exp(sink_grid - top)
    probs = (weights / total).astype(jnp.bfloat16)
    mixed = jnp.einsum(
        "bkgqs,bskd->bqkgd", probs, band_values, preferred_element_type=jnp.float32
    ).astype(jnp.bfloat16)
    row_log_weight_sum = (top + jnp.log(total))[..., 0]
    return (
        mixed.reshape(rows, kv_heads * group * HEAD_SIZE),
        row_log_weight_sum.transpose(1, 2, 0, 3).reshape(kv_heads * group, rows),
    )


def pool_branch(pool_rows, pool_tail, mixing, scales, group_start, first_pos):
    rows = pool_rows.shape[0]
    columns = pool_rows.shape[1]
    pool_reach = max(POOL_SPANS)
    extended = jnp.concatenate([pool_tail, pool_rows], 0).astype(jnp.float32)
    group_index = group_start + jnp.arange(columns) // POOL_CH
    span_table = jnp.array(POOL_SPANS, jnp.int32)
    matches = group_index[:, None] == jnp.arange(len(POOL_SPANS))[None, :]
    span_of_col = jnp.sum(jnp.where(matches, span_table[None, :], 0), axis=1)
    trailing = jnp.zeros((rows, columns), jnp.float32)
    for lag in range(pool_reach):
        trailing = trailing + jnp.where(
            lag < span_of_col[None, :], extended[pool_reach - lag : pool_reach - lag + rows], 0.0
        )
    position = first_pos + jnp.arange(rows)
    count = jnp.minimum(position[:, None] + 1, span_of_col[None, :]).astype(jnp.float32)
    centred = (trailing / count - extended[pool_reach:]).astype(jnp.bfloat16)
    grouped = centred.reshape(rows, columns // POOL_CH, POOL_CH)
    product = jnp.einsum(
        "rgc,gcd->rgd", grouped, mixing, preferred_element_type=jnp.float32
    ).reshape(rows, columns)
    return (product * scales).astype(jnp.bfloat16)


def local(
    tokens,
    norm_gain,
    query_weight,
    key_matrix,
    value_matrix,
    pool_in_weight,
    head_sink_logit,
    pool_mix,
    pool_gain,
    attn_out_weight,
    pool_out_weight,
):
    tp_index = lax.axis_index("tp")
    sp_index = lax.axis_index("sp")
    q_cols = query_weight.shape[1]
    kv_cols = key_matrix.shape[1]
    pool_cols = pool_in_weight.shape[1]
    q_heads = q_cols // HEAD_SIZE
    kv_heads = kv_cols // HEAD_SIZE
    groups_dev = pool_cols // POOL_CH
    full_query, full_key, full_value, full_pool = (
        lax.all_gather(query_weight, "sp", axis=0, tiled=True),
        lax.all_gather(key_matrix, "sp", axis=0, tiled=True),
        lax.all_gather(value_matrix, "sp", axis=0, tiled=True),
        lax.all_gather(pool_in_weight, "sp", axis=0, tiled=True),
    )
    values_f = lax.all_gather(tokens[0], "tp", axis=0, tiled=True).astype(jnp.float32)
    scale = lax.rsqrt(jnp.mean(values_f * values_f, axis=-1, keepdims=True) + EPSILON)
    normed = (values_f * scale * norm_gain).astype(jnp.bfloat16)
    outputs = [
        jnp.dot(normed, weight, preferred_element_type=jnp.float32).astype(jnp.bfloat16)
        for weight in (full_query, full_key, full_value, full_pool)
    ]
    projected = jnp.concatenate(outputs, axis=1)
    rows = projected.shape[0]
    first_pos = sp_index * rows
    query_rows = projected[:, :q_cols]
    key_rows = projected[:, q_cols : q_cols + kv_cols]
    value_rows = projected[:, q_cols + kv_cols : q_cols + 2 * kv_cols]
    pool_rows = projected[:, q_cols + 2 * kv_cols :]
    pool_reach = max(POOL_SPANS)
    sinks = lax.dynamic_slice_in_dim(head_sink_logit, tp_index * q_heads, q_heads, 0)
    mixing = lax.dynamic_slice_in_dim(pool_mix, tp_index * groups_dev, groups_dev, 0)
    scales = lax.dynamic_slice_in_dim(pool_gain, tp_index * pool_cols, pool_cols, 0)
    key_tail, value_tail, pool_tail = passed_along(
        (key_rows[rows - WINDOW :], value_rows[rows - WINDOW :], pool_rows[rows - pool_reach :]),
        "sp",
        1,
    )
    attn_part, log_part = windowed_attend(
        query_rows,
        key_rows,
        value_rows,
        key_tail,
        value_tail,
        sinks,
        kv_heads,
        q_heads // kv_heads,
        first_pos,
    )
    pool_part = pool_branch(pool_rows, pool_tail, mixing, scales, tp_index * groups_dev, first_pos)
    half_attn, half_pool = (
        lax.all_gather(attn_out_weight, "sp", axis=1, tiled=True),
        lax.all_gather(pool_out_weight, "sp", axis=1, tiled=True),
    )
    result = lax.psum_scatter(
        jnp.dot(attn_part, half_attn, preferred_element_type=jnp.float32)
        + jnp.dot(pool_part, half_pool, preferred_element_type=jnp.float32),
        "tp",
        scatter_dimension=0,
        tiled=True,
    ).astype(jnp.bfloat16)
    return (result[None], log_part[None])


LANES = 128
TILE = 16
X_LAG, Y_LAG, LEAD = 2, 4, 2
CUTS, FAR_LAG = 1, 1
MESH_ID = pl.DeviceIdType.MESH


def nearest(n, step, me):
    tables = [sorted((j for j in range(n) if j != z), key=lambda j: (abs(j - z), j)) for z in range(n)]
    shard = jnp.int32(tables[0][step])
    for z in range(1, n):
        shard = jnp.where(me == z, tables[z][step], shard)
    return shard


def layer_kernel(
    n,
    sinks,
    tokens,
    gain,
    wq,
    wk,
    wv,
    wp,
    mix,
    pool_gain,
    wao,
    wpo,
    out,
    log_out,
    held,
    tok,
    normed,
    proj,
    kv,
    pool_ext,
    mixed,
    mix_own,
    mine,
    sent,
    got,
    z_send,
    x_send,
    y_send,
    z_recv,
    x_recv,
    y_recv,
    load_sem,
    tok_sem,
    halo_send,
    halo_recv,
    sum_send,
    sum_recv,
):
    me = lax.axis_index("sp")
    f = lax.axis_index("fs")
    c = lax.axis_index("tp")
    f32 = jnp.float32
    half = tokens.shape[0]
    rows = 2 * half
    depth = wq.shape[0]
    n_in = (wq.shape[1] + wk.shape[1] + wv.shape[1] + wp.shape[1]) // LANES
    out_tiles = wao.shape[1] // LANES
    n_blocks = n_in + 2 * out_tiles
    steps = n_blocks // 3 * CUTS
    sources = [wk, wv] + [wq.at[:, pl.ds(i * LANES, LANES)] for i in range(wq.shape[1] // LANES)]
    sources += [wp.at[:, pl.ds(i * LANES, LANES)] for i in range(wp.shape[1] // LANES)]
    for i in range(out_tiles):
        sources += [w.at[:, pl.ds(i * LANES, LANES)] for w in (wao, wpo)]
    z_part = lax.rem(f, 3)
    beside = f + 1 - 2 * lax.rem(f, 2)
    across = lax.rem(f + 2, 4)
    x_part = lax.rem(beside, 3)
    y_part = 3 - z_part - x_part
    relays = (f == 0) | (f == 3)
    y_out = jnp.where(relays, x_part, z_part)
    up, down = me + 1, me - 1
    has_up, has_down = me < n - 1, me > 0

    def load(i):
        return pltpu.make_async_copy(sources[i], held.at[me, i], load_sem.at[i])

    for i in range(n_blocks):
        load(i).start()
    own_rows = pl.ds(pl.multiple_of(c * half, half), half)
    tok_load = pltpu.make_async_copy(tokens, tok.at[own_rows], tok_sem.at[2])
    tok_load.start()
    groups = mix_own.shape[0]
    mix_load = pltpu.make_async_copy(mix.at[pl.ds(c * groups, groups)], mix_own, tok_sem.at[3])
    mix_load.start()

    barrier = pltpu.get_barrier_semaphore()
    pl.semaphore_signal(barrier, inc=1, device_id={"tp": 1 - c}, device_id_type=MESH_ID)
    pl.semaphore_signal(barrier, inc=1, device_id={"fs": beside}, device_id_type=MESH_ID)
    pl.semaphore_signal(barrier, inc=1, device_id={"fs": across}, device_id_type=MESH_ID)

    @pl.when(has_up)
    def _():
        pl.semaphore_signal(barrier, inc=1, device_id={"sp": up}, device_id_type=MESH_ID)

    @pl.when(has_down)
    def _():
        pl.semaphore_signal(barrier, inc=1, device_id={"sp": down}, device_id_type=MESH_ID)

    pl.semaphore_wait(barrier, 3 + has_up.astype(jnp.int32) + has_down.astype(jnp.int32))

    tok_send = pltpu.make_async_remote_copy(
        tokens, tok.at[own_rows], tok_sem.at[0], tok_sem.at[1],
        device_id={"tp": 1 - c}, device_id_type=MESH_ID,
    )
    tok_send.start()

    def hop(s, j, part, send, recv, to):
        size = depth // CUTS
        block = held.at[j, 3 * (s // CUTS) + part, pl.ds(s % CUTS * size, size)]
        return pltpu.make_async_remote_copy(
            block, block, send, recv.at[s, j], device_id=to, device_id_type=MESH_ID
        )

    def z_hop(s, j, way):
        to = jnp.where(way == 0, up, down)
        return hop(s, j, z_part, z_send.at[way, s, j], z_recv, {"sp": to})

    def x_hop(s, j):
        return hop(s, j, z_part, x_send.at[s, j], x_recv, {"fs": beside})

    def y_hop(s, j):
        return hop(s, j, y_out, y_send.at[s, j], y_recv, {"fs": across})

    def onward(j):
        return jnp.where(j < me, 0, 1), ((j < me) & has_up) | ((j > me) & has_down)

    def own_send(s, finish=False):
        @pl.when(has_up)
        def _():
            cp = z_hop(s, me, 0)
            cp.wait_send() if finish else cp.start()

        @pl.when(has_down)
        def _():
            cp = z_hop(s, me, 1)
            cp.wait_send() if finish else cp.start()

    slots = [(s, k) for s in range(steps) for k in range(n - 1)]
    slots.sort(key=lambda slot: (slot[0] + FAR_LAG * slot[1], slot))
    shard = [nearest(n, k, me) for k in range(n - 1)]

    def z_step(t):
        s, k = slots[t]
        j = shard[k]
        if k == 0 and s + LEAD < steps:

            @pl.when(has_up & has_down)
            def _():
                own_send(s + LEAD)

        z_hop(s, j, 0).wait_recv()
        way, more = onward(j)

        @pl.when(more)
        def _():
            z_hop(s, j, way).start()

        x_hop(s, j).start()

    def x_step(t):
        s, k = slots[t]
        hop(s, shard[k], x_part, x_send.at[s, shard[k]], x_recv, {"fs": beside}).wait_recv()
        y_hop(s, shard[k]).start()

    def y_step(t):
        s, k = slots[t]
        hop(s, shard[k], y_part, y_send.at[s, shard[k]], y_recv, {"fs": across}).wait_recv()

    for i in range(n_blocks):
        load(i).wait()
        if i % 3 == 2:
            for s in range(i // 3 * CUTS, (i // 3 + 1) * CUTS):
                if s < LEAD:
                    own_send(s)
                else:

                    @pl.when(jnp.logical_not(has_up & has_down))
                    def _():
                        own_send(s)


    def norm_rows(r, size):
        v = tok[pl.ds(r, size), :].astype(f32)
        scale = lax.rsqrt(jnp.mean(v * v, axis=-1, keepdims=True) + EPSILON)
        normed[pl.ds(r, size), :] = (v * scale * gain[...]).astype(jnp.bfloat16)

    def norm_all():
        tok_load.wait()
        tok_send.wait()
        mix_load.wait()
        chunk = 32

        @pl.loop(0, rows // chunk)
        def _(i):
            norm_rows(pl.multiple_of(i * chunk, chunk), chunk)

    def project(pair):
        acc = None
        for j in range(n):
            w = jnp.concatenate([held[j, 2 * pair], held[j, 2 * pair + 1]], axis=1)
            term = jnp.dot(normed[:, j * depth : (j + 1) * depth], w, preferred_element_type=f32)
            acc = term if acc is None else acc + term
        return acc.astype(jnp.bfloat16)

    def halo_kv():
        return pltpu.make_async_remote_copy(
            kv.at[pl.ds(rows, WINDOW)], kv.at[pl.ds(0, WINDOW)], halo_send.at[0], halo_recv.at[0],
            device_id={"sp": up}, device_id_type=MESH_ID,
        )

    def halo_pool(g):
        return pltpu.make_async_remote_copy(
            pool_ext.at[g, pl.ds(rows, TILE)], pool_ext.at[g, pl.ds(0, TILE)],
            halo_send.at[1 + g], halo_recv.at[1 + g],
            device_id={"sp": up}, device_id_type=MESH_ID,
        )

    def first_zero(store):
        @pl.when(me == 0)
        def _():
            store()

    def project_kv():
        kv[pl.ds(WINDOW, rows), :] = project(0)

        @pl.when(has_up)
        def _():
            halo_kv().start()

        def zero():
            kv[pl.ds(0, WINDOW), :] = jnp.zeros((WINDOW, kv.shape[1]), kv.dtype)

        first_zero(zero)

    def project_q(g):
        proj[g] = project(1 + g)

    kv_cols = wk.shape[1]
    kv_heads = kv_cols // HEAD_SIZE
    group = wq.shape[1] // HEAD_SIZE // kv_heads

    def project_pool(g):
        pool_ext[g, pl.ds(TILE, rows), :] = project(1 + kv_heads + g)

        @pl.when(has_up)
        def _():
            halo_pool(g).start()

        def zero():
            pool_ext[g, pl.ds(0, TILE), :] = jnp.zeros((TILE, POOL_CH), pool_ext.dtype)

        first_zero(zero)

    def kv_arrived():
        @pl.when(has_down)
        def _():
            halo_kv().wait_recv()

    def attend(b):
        base = b * WINDOW
        lane = lax.broadcasted_iota(jnp.int32, (WINDOW, LANES), 1)
        logs = jnp.zeros((WINDOW, LANES), f32)
        i_pos = lax.broadcasted_iota(jnp.int32, (WINDOW, 2 * WINDOW), 0)
        k_pos = lax.broadcasted_iota(jnp.int32, (WINDOW, 2 * WINDOW), 1)
        allowed = (k_pos > i_pos) & (k_pos <= i_pos + WINDOW)
        allowed = allowed & (k_pos + (me * rows + base - WINDOW) >= 0)
        for g in range(kv_heads):
            band = kv[pl.ds(base, 2 * WINDOW), :]
            keys = band[:, g * HEAD_SIZE : (g + 1) * HEAD_SIZE]
            vals = band[:, kv_cols + g * HEAD_SIZE : kv_cols + (g + 1) * HEAD_SIZE]
            q = proj[g, pl.ds(base, WINDOW), :]
            q = jnp.concatenate([q[:, h * HEAD_SIZE : (h + 1) * HEAD_SIZE] for h in range(group)], axis=0)
            scores = lax.dot_general(q, keys, (((1,), (1,)), ((), ())), preferred_element_type=f32)
            probs = []
            for h in range(group):
                head = g * group + h
                sink = sinks[c * kv_heads * group + head]
                sc = jnp.where(allowed, scores[h * WINDOW : (h + 1) * WINDOW] * HEAD_SIZE**-0.5, -jnp.inf)
                top = jnp.maximum(jnp.max(sc, axis=-1, keepdims=True), sink)
                w = jnp.exp(sc - top)
                total = jnp.sum(w, axis=-1, keepdims=True) + jnp.exp(sink - top)
                probs.append((w * (1.0 / total)).astype(jnp.bfloat16))
                logs = jnp.where(lane == head, top + jnp.log(total), logs)
            res = jnp.dot(jnp.concatenate(probs, axis=0), vals, preferred_element_type=f32)
            res = jnp.concatenate([res[h * WINDOW : (h + 1) * WINDOW] for h in range(group)], axis=1)
            mixed[g, pl.ds(base, WINDOW), :] = res.astype(jnp.bfloat16)
        log_out[:, pl.ds(base, WINDOW)] = jnp.transpose(logs)[: kv_heads * group]

    def pool(g):
        @pl.when(has_down)
        def _():
            halo_pool(g).wait_recv()

        index = c * groups + g
        run = pool_ext[g].astype(f32)
        own = run[TILE:]
        trailing = jnp.zeros_like(run)
        span_here = jnp.int32(0)
        reach = 1
        for at, span in enumerate(POOL_SPANS):
            while reach < span:
                run = run + pltpu.roll(run, reach, 0)
                reach *= 2
            trailing = jnp.where(index == at, run, trailing)
            span_here = jnp.where(index == at, span, span_here)
        pos = me * rows + lax.broadcasted_iota(jnp.int32, (rows, 1), 0)
        count = jnp.minimum(pos + 1, span_here).astype(f32)
        centred = (trailing[TILE:] / count - own).astype(jnp.bfloat16)
        product = jnp.dot(centred, mix_own[g], preferred_element_type=f32)
        mixed[kv_heads + g] = (product * pool_gain[index]).astype(jnp.bfloat16)

    n_pairs = out_tiles // 2

    def sum_hop(slot):
        return pltpu.make_async_remote_copy(
            sent.at[slot], got.at[slot], sum_send.at[slot], sum_recv.at[slot],
            device_id={"tp": 1 - c}, device_id_type=MESH_ID,
        )

    def out_project(j, pair):
        slot = j * n_pairs + pair
        acc = None
        for side in range(2):
            first = n_in + 4 * pair + side
            w = jnp.concatenate([held[j, first], held[j, first + 2]], axis=1)
            parts = mixed.shape[0] // 2
            a = jnp.concatenate([mixed[side * parts + i] for i in range(parts)], axis=1)
            term = jnp.dot(a, w, preferred_element_type=f32)
            acc = term if acc is None else acc + term
        low, high = acc[:half], acc[half:]
        mine[slot] = jnp.where(c == 0, low, high)
        sent[slot] = jnp.where(c == 0, high, low)
        sum_hop(slot).start()

    def finish(j, pair):
        slot = j * n_pairs + pair
        sum_hop(slot).wait()
        wide = 2 * LANES
        cols = pl.ds(pl.multiple_of(slot * wide, wide), wide)
        out[:, cols] = (mine[slot] + got[slot]).astype(jnp.bfloat16)

    tasks = {}

    def ready(block):
        return slots.index((block // 3 * CUTS + CUTS - 1, n - 2))

    def at(t, task, *args):
        tasks.setdefault(min(t, len(slots) - 1), []).append((task, args))

    at(-1, norm_all)
    at(ready(1), project_kv)
    for g in range(kv_heads):
        at(ready(2 * g + 3), project_q, g)
    last = ready(2 * kv_heads + 1) + 1
    at(last, kv_arrived)
    for b in range(rows // WINDOW):
        at(last + b // 2, attend, b)
    for g in range(groups):
        at(ready(2 * (1 + kv_heads + g) + 1), project_pool, g)
    for g in range(groups):
        at(ready(2 * (kv_heads + groups) + 1) + (g + 1) // 2, pool, g)
    base_slot = ready(n_in - 1) + 1
    order = []
    for pair in range(n_pairs):
        at(base_slot, out_project, me, pair)
        order.append((base_slot, me, pair))
    for k in range(n - 1):
        for pair in range(n_pairs):
            when = slots.index(((n_in + 4 * pair + 3) // 3 * CUTS + CUTS - 1, k))
            at(max(when, base_slot), out_project, shard[k], pair)
            order.append((max(when, base_slot), shard[k], pair))

    late = []
    for when, j, pair in order:
        if when + 2 < len(slots) - 1:
            at(when + 2, finish, j, pair)
        else:
            late.append((j, pair))
    total_slots = len(slots)
    for task, args in tasks.pop(-1, ()):
        task(*args)
    for t in range(total_slots + Y_LAG):
        if t < total_slots:
            z_step(t)
        if 0 <= t - X_LAG < total_slots:
            x_step(t - X_LAG)
        if t >= Y_LAG:
            y_step(t - Y_LAG)
            for task, args in tasks.pop(t - Y_LAG, ()):
                task(*args)
    for j, pair in late:
        finish(j, pair)

    for s in range(steps):
        own_send(s, finish=True)
    for s, k in slots:
        way, more = onward(shard[k])

        @pl.when(more)
        def _():
            z_hop(s, shard[k], way).wait_send()

        x_hop(s, shard[k]).wait_send()
        y_hop(s, shard[k]).wait_send()

    @pl.when(has_up)
    def _():
        halo_kv().wait_send()
        for g in range(groups):
            halo_pool(g).wait_send()


def fused_local(
    n,
    tokens,
    norm_gain,
    query_weight,
    key_matrix,
    value_matrix,
    pool_in_weight,
    head_sink_logit,
    pool_mix,
    pool_gain,
    attn_out_weight,
    pool_out_weight,
):
    _, half, width = tokens.shape
    rows = 2 * half
    depth, q_cols = query_weight.shape
    kv_cols = key_matrix.shape[1]
    pool_cols = pool_in_weight.shape[1]
    heads = q_cols // HEAD_SIZE
    kv_heads = kv_cols // HEAD_SIZE
    groups = pool_cols // POOL_CH
    n_in = (q_cols + 2 * kv_cols + pool_cols) // LANES
    n_blocks = n_in + 2 * attn_out_weight.shape[1] // LANES
    steps = n_blocks // 3 * CUTS
    pieces = n * attn_out_weight.shape[1] // (2 * LANES)
    bf16, f32 = jnp.bfloat16, jnp.float32
    dma = pltpu.SemaphoreType.DMA
    hbm = pl.BlockSpec(memory_space=pl.ANY)
    vmem = pl.BlockSpec(memory_space=pltpu.VMEM)
    smem = pl.BlockSpec(memory_space=pltpu.SMEM)
    mixed, logs = pl.pallas_call(
        functools.partial(layer_kernel, n),
        out_shape=(
            jax.ShapeDtypeStruct((half, width), bf16),
            jax.ShapeDtypeStruct((heads, rows), f32),
        ),
        in_specs=[smem, hbm, vmem, hbm, hbm, hbm, hbm, hbm, vmem, hbm, hbm],
        out_specs=(vmem, vmem),
        scratch_shapes=[
            pltpu.VMEM((n, n_blocks, depth, LANES), bf16),
            pltpu.VMEM((rows, width), bf16),
            pltpu.VMEM((rows, width), bf16),
            pltpu.VMEM((kv_heads, rows, 2 * LANES), bf16),
            pltpu.VMEM((WINDOW + rows, 2 * kv_cols), bf16),
            pltpu.VMEM((groups, TILE + rows, POOL_CH), bf16),
            pltpu.VMEM((kv_heads + groups, rows, 2 * LANES), bf16),
            pltpu.VMEM((groups, POOL_CH, POOL_CH), bf16),
            pltpu.VMEM((pieces, half, 2 * LANES), f32),
            pltpu.VMEM((pieces, half, 2 * LANES), f32),
            pltpu.VMEM((pieces, half, 2 * LANES), f32),
            dma((2, steps, n)),
            dma((steps, n)),
            dma((steps, n)),
            dma((steps, n)),
            dma((steps, n)),
            dma((steps, n)),
            dma((n_blocks,)),
            dma((4,)),
            dma((1 + groups,)),
            dma((1 + groups,)),
            dma((pieces,)),
            dma((pieces,)),
        ],
        compiler_params=pltpu.CompilerParams(
            collective_id=0, has_side_effects=True, vmem_limit_bytes=60 * 1024 * 1024
        ),
    )(
        head_sink_logit,
        tokens[0],
        norm_gain.reshape(1, width),
        query_weight,
        key_matrix,
        value_matrix,
        pool_in_weight,
        pool_mix,
        pool_gain.reshape(-1, 1, POOL_CH),
        attn_out_weight,
        pool_out_weight,
    )
    return mixed[None], logs[None]


def fits(mesh, tokens, query_weight, key_matrix, pool_in_weight, attn_out_weight):
    n, f, c = mesh.shape["sp"], mesh.shape["fs"], mesh.shape["tp"]
    depth = query_weight.shape[0] // n
    rows = tokens.shape[1] // n
    q_cols, kv_cols, pool_cols = (w.shape[1] // c for w in (query_weight, key_matrix, pool_in_weight))
    tiles = attn_out_weight.shape[1] // n // LANES
    blocks = (q_cols + 2 * kv_cols + pool_cols) // LANES + 2 * tiles
    return (
        2 <= n <= 4
        and f == 4
        and c == 2
        and tokens.shape[0] == f
        and rows % WINDOW == 0
        and kv_cols == LANES
        and q_cols == 2 * LANES * (kv_cols // HEAD_SIZE)
        and pool_cols == q_cols
        and POOL_CH == 2 * LANES
        and attn_out_weight.shape[1] % (n * 2 * LANES) == 0
        and attn_out_weight.shape[0] // c == depth
        and depth % LANES == 0
        and blocks % 3 == 0
    )


def solution(mesh):
    in_specs = (
        P("fs", ("sp", "tp"), None),
        P(),
        P("sp", "tp"),
        P("sp", "tp"),
        P("sp", "tp"),
        P("sp", "tp"),
        P(),
        P(),
        P(),
        P("tp", "sp"),
        P("tp", "sp"),
    )
    out_specs = (P("fs", ("sp", "tp"), None), P("fs", "tp", "sp"))

    def step(*args):
        fused = fits(mesh, args[0], args[2], args[3], args[5], args[9])
        body = functools.partial(fused_local, mesh.shape["sp"]) if fused else local
        mapped = jax.shard_map(body, mesh=mesh, in_specs=in_specs, out_specs=out_specs, check_vma=False)
        return mapped(*args)

    return step
```

```python
import functools

import jax
import jax.numpy as jnp
from jax import lax
from jax.experimental import pallas as pl
from jax.experimental.pallas import tpu as pltpu
from jax.sharding import PartitionSpec as P

HEAD_SIZE = 64
WINDOW = 128
POOL_CH = 256


EPSILON = 1e-06
POOL_SPANS = (2, 4, 8, 16)


def passed_along(shard, axis, by):
    size = lax.axis_size(axis)
    pairs = [(i, i + by) for i in range(size) if 0 <= i + by < size]
    return lax.ppermute(shard, axis, pairs)


def windowed_attend(
    query_rows, key_rows, value_rows, key_tail, value_tail, sinks, kv_heads, group, first_pos
):
    rows = query_rows.shape[0]
    blocks = rows // WINDOW
    width = key_rows.shape[1]
    ext_keys = jnp.concatenate([key_tail, key_rows], 0)
    ext_values = jnp.concatenate([value_tail, value_rows], 0)

    def banded(table):
        return jnp.concatenate(
            [
                table[:rows].reshape(blocks, WINDOW, width),
                table[WINDOW:].reshape(blocks, WINDOW, width),
            ],
            axis=1,
        )

    band_keys = banded(ext_keys).reshape(blocks, 2 * WINDOW, kv_heads, HEAD_SIZE)
    band_values = banded(ext_values).reshape(blocks, 2 * WINDOW, kv_heads, HEAD_SIZE)
    query_blocks = query_rows.reshape(blocks, WINDOW, kv_heads, group, HEAD_SIZE)
    scores = jnp.einsum(
        "bqkgd,bskd->bkgqs", query_blocks, band_keys, preferred_element_type=jnp.float32
    ) * HEAD_SIZE ** (-0.5)
    query_pos = first_pos + jnp.arange(rows).reshape(blocks, WINDOW, 1)
    key_pos = (
        first_pos
        - WINDOW
        + jnp.arange(blocks).reshape(blocks, 1, 1) * WINDOW
        + jnp.arange(2 * WINDOW).reshape(1, 1, 2 * WINDOW)
    )
    offset = query_pos - key_pos
    allowed = (offset >= 0) & (offset < WINDOW) & (key_pos >= 0)
    scores = jnp.where(allowed[:, None, None], scores, -jnp.inf)
    sink_grid = sinks.reshape(1, kv_heads, group, 1, 1)
    top = jnp.maximum(jnp.max(scores, axis=-1, keepdims=True), sink_grid)
    weights = jnp.exp(scores - top)
    total = jnp.sum(weights, axis=-1, keepdims=True) + jnp.exp(sink_grid - top)
    probs = (weights / total).astype(jnp.bfloat16)
    mixed = jnp.einsum(
        "bkgqs,bskd->bqkgd", probs, band_values, preferred_element_type=jnp.float32
    ).astype(jnp.bfloat16)
    row_log_weight_sum = (top + jnp.log(total))[..., 0]
    return (
        mixed.reshape(rows, kv_heads * group * HEAD_SIZE),
        row_log_weight_sum.transpose(1, 2, 0, 3).reshape(kv_heads * group, rows),
    )


def pool_branch(pool_rows, pool_tail, mixing, scales, group_start, first_pos):
    rows = pool_rows.shape[0]
    columns = pool_rows.shape[1]
    pool_reach = max(POOL_SPANS)
    extended = jnp.concatenate([pool_tail, pool_rows], 0).astype(jnp.float32)
    group_index = group_start + jnp.arange(columns) // POOL_CH
    span_table = jnp.array(POOL_SPANS, jnp.int32)
    matches = group_index[:, None] == jnp.arange(len(POOL_SPANS))[None, :]
    span_of_col = jnp.sum(jnp.where(matches, span_table[None, :], 0), axis=1)
    trailing = jnp.zeros((rows, columns), jnp.float32)
    for lag in range(pool_reach):
        trailing = trailing + jnp.where(
            lag < span_of_col[None, :], extended[pool_reach - lag : pool_reach - lag + rows], 0.0
        )
    position = first_pos + jnp.arange(rows)
    count = jnp.minimum(position[:, None] + 1, span_of_col[None, :]).astype(jnp.float32)
    centred = (trailing / count - extended[pool_reach:]).astype(jnp.bfloat16)
    grouped = centred.reshape(rows, columns // POOL_CH, POOL_CH)
    product = jnp.einsum(
        "rgc,gcd->rgd", grouped, mixing, preferred_element_type=jnp.float32
    ).reshape(rows, columns)
    return (product * scales).astype(jnp.bfloat16)


def local(
    tokens,
    norm_gain,
    query_weight,
    key_matrix,
    value_matrix,
    pool_in_weight,
    head_sink_logit,
    pool_mix,
    pool_gain,
    attn_out_weight,
    pool_out_weight,
):
    tp_index = lax.axis_index("tp")
    sp_index = lax.axis_index("sp")
    q_cols = query_weight.shape[1]
    kv_cols = key_matrix.shape[1]
    pool_cols = pool_in_weight.shape[1]
    q_heads = q_cols // HEAD_SIZE
    kv_heads = kv_cols // HEAD_SIZE
    groups_dev = pool_cols // POOL_CH
    full_query, full_key, full_value, full_pool = (
        lax.all_gather(query_weight, "sp", axis=0, tiled=True),
        lax.all_gather(key_matrix, "sp", axis=0, tiled=True),
        lax.all_gather(value_matrix, "sp", axis=0, tiled=True),
        lax.all_gather(pool_in_weight, "sp", axis=0, tiled=True),
    )
    values_f = lax.all_gather(tokens[0], "tp", axis=0, tiled=True).astype(jnp.float32)
    scale = lax.rsqrt(jnp.mean(values_f * values_f, axis=-1, keepdims=True) + EPSILON)
    normed = (values_f * scale * norm_gain).astype(jnp.bfloat16)
    outputs = [
        jnp.dot(normed, weight, preferred_element_type=jnp.float32).astype(jnp.bfloat16)
        for weight in (full_query, full_key, full_value, full_pool)
    ]
    projected = jnp.concatenate(outputs, axis=1)
    rows = projected.shape[0]
    first_pos = sp_index * rows
    query_rows = projected[:, :q_cols]
    key_rows = projected[:, q_cols : q_cols + kv_cols]
    value_rows = projected[:, q_cols + kv_cols : q_cols + 2 * kv_cols]
    pool_rows = projected[:, q_cols + 2 * kv_cols :]
    pool_reach = max(POOL_SPANS)
    sinks = lax.dynamic_slice_in_dim(head_sink_logit, tp_index * q_heads, q_heads, 0)
    mixing = lax.dynamic_slice_in_dim(pool_mix, tp_index * groups_dev, groups_dev, 0)
    scales = lax.dynamic_slice_in_dim(pool_gain, tp_index * pool_cols, pool_cols, 0)
    key_tail, value_tail, pool_tail = passed_along(
        (key_rows[rows - WINDOW :], value_rows[rows - WINDOW :], pool_rows[rows - pool_reach :]),
        "sp",
        1,
    )
    attn_part, log_part = windowed_attend(
        query_rows,
        key_rows,
        value_rows,
        key_tail,
        value_tail,
        sinks,
        kv_heads,
        q_heads // kv_heads,
        first_pos,
    )
    pool_part = pool_branch(pool_rows, pool_tail, mixing, scales, tp_index * groups_dev, first_pos)
    half_attn, half_pool = (
        lax.all_gather(attn_out_weight, "sp", axis=1, tiled=True),
        lax.all_gather(pool_out_weight, "sp", axis=1, tiled=True),
    )
    result = lax.psum_scatter(
        jnp.dot(attn_part, half_attn, preferred_element_type=jnp.float32)
        + jnp.dot(pool_part, half_pool, preferred_element_type=jnp.float32),
        "tp",
        scatter_dimension=0,
        tiled=True,
    ).astype(jnp.bfloat16)
    return (result[None], log_part[None])


LANES = 128
TILE = 16
X_LAG, Y_LAG, LEAD = 2, 6, 2
CUTS, FAR_LAG = 1, 0
MESH_ID = pl.DeviceIdType.MESH


def nearest(n, step, me):
    tables = [sorted((j for j in range(n) if j != z), key=lambda j: (abs(j - z), j)) for z in range(n)]
    shard = jnp.int32(tables[0][step])
    for z in range(1, n):
        shard = jnp.where(me == z, tables[z][step], shard)
    return shard


def layer_kernel(
    n,
    sinks,
    tokens,
    gain,
    wq,
    wk,
    wv,
    wp,
    mix,
    pool_gain,
    wao,
    wpo,
    out,
    log_out,
    held,
    tok,
    normed,
    proj,
    kv,
    pool_ext,
    mixed,
    mix_own,
    mine,
    sent,
    got,
    z_send,
    x_send,
    y_send,
    z_recv,
    x_recv,
    y_recv,
    load_sem,
    tok_sem,
    halo_send,
    halo_recv,
    sum_send,
    sum_recv,
):
    me = lax.axis_index("sp")
    f = lax.axis_index("fs")
    c = lax.axis_index("tp")
    f32 = jnp.float32
    half = tokens.shape[0]
    rows = 2 * half
    depth = wq.shape[0]
    n_in = (wq.shape[1] + wk.shape[1] + wv.shape[1] + wp.shape[1]) // LANES
    out_tiles = wao.shape[1] // LANES
    n_blocks = n_in + 2 * out_tiles
    steps = n_blocks // 3 * CUTS
    sources = [wk, wv] + [wq.at[:, pl.ds(i * LANES, LANES)] for i in range(wq.shape[1] // LANES)]
    sources += [wp.at[:, pl.ds(i * LANES, LANES)] for i in range(wp.shape[1] // LANES)]
    for i in range(out_tiles):
        sources += [w.at[:, pl.ds(i * LANES, LANES)] for w in (wao, wpo)]
    z_part = lax.rem(f, 3)
    beside = f + 1 - 2 * lax.rem(f, 2)
    across = lax.rem(f + 2, 4)
    x_part = lax.rem(beside, 3)
    y_part = 3 - z_part - x_part
    relays = (f == 0) | (f == 3)
    y_out = jnp.where(relays, x_part, z_part)
    up, down = me + 1, me - 1
    has_up, has_down = me < n - 1, me > 0

    def load(i):
        return pltpu.make_async_copy(sources[i], held.at[me, i], load_sem.at[i])

    for i in range(n_blocks):
        load(i).start()
    own_rows = pl.ds(pl.multiple_of(c * half, half), half)
    tok_load = pltpu.make_async_copy(tokens, tok.at[own_rows], tok_sem.at[2])
    tok_load.start()
    groups = mix_own.shape[0]
    mix_load = pltpu.make_async_copy(mix.at[pl.ds(c * groups, groups)], mix_own, tok_sem.at[3])
    mix_load.start()

    barrier = pltpu.get_barrier_semaphore()
    pl.semaphore_signal(barrier, inc=1, device_id={"tp": 1 - c}, device_id_type=MESH_ID)
    pl.semaphore_signal(barrier, inc=1, device_id={"fs": beside}, device_id_type=MESH_ID)
    pl.semaphore_signal(barrier, inc=1, device_id={"fs": across}, device_id_type=MESH_ID)

    @pl.when(has_up)
    def _():
        pl.semaphore_signal(barrier, inc=1, device_id={"sp": up}, device_id_type=MESH_ID)

    @pl.when(has_down)
    def _():
        pl.semaphore_signal(barrier, inc=1, device_id={"sp": down}, device_id_type=MESH_ID)

    pl.semaphore_wait(barrier, 3 + has_up.astype(jnp.int32) + has_down.astype(jnp.int32))

    tok_send = pltpu.make_async_remote_copy(
        tokens, tok.at[own_rows], tok_sem.at[0], tok_sem.at[1],
        device_id={"tp": 1 - c}, device_id_type=MESH_ID,
    )
    tok_send.start()

    def hop(s, j, part, send, recv, to):
        size = depth // CUTS
        block = held.at[j, 3 * (s // CUTS) + part, pl.ds(s % CUTS * size, size)]
        return pltpu.make_async_remote_copy(
            block, block, send, recv.at[s, j], device_id=to, device_id_type=MESH_ID
        )

    def z_hop(s, j, way):
        to = jnp.where(way == 0, up, down)
        return hop(s, j, z_part, z_send.at[way, s, j], z_recv, {"sp": to})

    def x_hop(s, j):
        return hop(s, j, z_part, x_send.at[s, j], x_recv, {"fs": beside})

    def y_hop(s, j):
        return hop(s, j, y_out, y_send.at[s, j], y_recv, {"fs": across})

    def onward(j):
        return jnp.where(j < me, 0, 1), ((j < me) & has_up) | ((j > me) & has_down)

    def own_send(s, finish=False):
        @pl.when(has_up)
        def _():
            cp = z_hop(s, me, 0)
            cp.wait_send() if finish else cp.start()

        @pl.when(has_down)
        def _():
            cp = z_hop(s, me, 1)
            cp.wait_send() if finish else cp.start()

    slots = [(s, k) for s in range(steps) for k in range(n - 1)]
    slots.sort(key=lambda slot: (slot[0] + FAR_LAG * slot[1], slot))
    shard = [nearest(n, k, me) for k in range(n - 1)]

    def z_step(t):
        s, k = slots[t]
        j = shard[k]
        if k == 0 and s + LEAD < steps:

            @pl.when(has_up & has_down)
            def _():
                own_send(s + LEAD)

        z_hop(s, j, 0).wait_recv()
        way, more = onward(j)

        @pl.when(more)
        def _():
            z_hop(s, j, way).start()

        x_hop(s, j).start()

        @pl.when(jnp.logical_not(relays))
        def _():
            y_hop(s, j).start()


    def x_step(t):
        s, k = slots[t]
        hop(s, shard[k], x_part, x_send.at[s, shard[k]], x_recv, {"fs": beside}).wait_recv()

        @pl.when(relays)
        def _():
            y_hop(s, shard[k]).start()


    def y_step(t):
        s, k = slots[t]
        hop(s, shard[k], y_part, y_send.at[s, shard[k]], y_recv, {"fs": across}).wait_recv()

    for i in range(n_blocks):
        load(i).wait()
        if i % 3 == 2:
            for s in range(i // 3 * CUTS, (i // 3 + 1) * CUTS):
                if s < LEAD:
                    own_send(s)
                else:

                    @pl.when(jnp.logical_not(has_up & has_down))
                    def _():
                        own_send(s)


    def norm_rows(r, size):
        v = tok[pl.ds(r, size), :].astype(f32)
        scale = lax.rsqrt(jnp.mean(v * v, axis=-1, keepdims=True) + EPSILON)
        normed[pl.ds(r, size), :] = (v * scale * gain[...]).astype(jnp.bfloat16)

    def norm_all():
        tok_load.wait()
        tok_send.wait()
        mix_load.wait()
        chunk = 32

        @pl.loop(0, rows // chunk)
        def _(i):
            norm_rows(pl.multiple_of(i * chunk, chunk), chunk)

    def project(pair):
        acc = None
        for j in range(n):
            w = jnp.concatenate([held[j, 2 * pair], held[j, 2 * pair + 1]], axis=1)
            term = jnp.dot(normed[:, j * depth : (j + 1) * depth], w, preferred_element_type=f32)
            acc = term if acc is None else acc + term
        return acc.astype(jnp.bfloat16)

    def halo_kv():
        return pltpu.make_async_remote_copy(
            kv.at[pl.ds(rows, WINDOW)], kv.at[pl.ds(0, WINDOW)], halo_send.at[0], halo_recv.at[0],
            device_id={"sp": up}, device_id_type=MESH_ID,
        )

    def halo_pool(g):
        return pltpu.make_async_remote_copy(
            pool_ext.at[g, pl.ds(rows, TILE)], pool_ext.at[g, pl.ds(0, TILE)],
            halo_send.at[1 + g], halo_recv.at[1 + g],
            device_id={"sp": up}, device_id_type=MESH_ID,
        )

    def first_zero(store):
        @pl.when(me == 0)
        def _():
            store()

    def project_kv():
        kv[pl.ds(WINDOW, rows), :] = project(0)

        @pl.when(has_up)
        def _():
            halo_kv().start()

        def zero():
            kv[pl.ds(0, WINDOW), :] = jnp.zeros((WINDOW, kv.shape[1]), kv.dtype)

        first_zero(zero)

    def project_q(g):
        proj[g] = project(1 + g)

    kv_cols = wk.shape[1]
    kv_heads = kv_cols // HEAD_SIZE
    group = wq.shape[1] // HEAD_SIZE // kv_heads

    def project_pool(g):
        pool_ext[g, pl.ds(TILE, rows), :] = project(1 + kv_heads + g)

        @pl.when(has_up)
        def _():
            halo_pool(g).start()

        def zero():
            pool_ext[g, pl.ds(0, TILE), :] = jnp.zeros((TILE, POOL_CH), pool_ext.dtype)

        first_zero(zero)

    def kv_arrived():
        @pl.when(has_down)
        def _():
            halo_kv().wait_recv()

    def attend(b):
        base = b * WINDOW
        lane = lax.broadcasted_iota(jnp.int32, (WINDOW, LANES), 1)
        logs = jnp.zeros((WINDOW, LANES), f32)
        i_pos = lax.broadcasted_iota(jnp.int32, (WINDOW, 2 * WINDOW), 0)
        k_pos = lax.broadcasted_iota(jnp.int32, (WINDOW, 2 * WINDOW), 1)
        allowed = (k_pos > i_pos) & (k_pos <= i_pos + WINDOW)
        allowed = allowed & (k_pos + (me * rows + base - WINDOW) >= 0)
        for g in range(kv_heads):
            band = kv[pl.ds(base, 2 * WINDOW), :]
            keys = band[:, g * HEAD_SIZE : (g + 1) * HEAD_SIZE]
            vals = band[:, kv_cols + g * HEAD_SIZE : kv_cols + (g + 1) * HEAD_SIZE]
            q = proj[g, pl.ds(base, WINDOW), :]
            q = jnp.concatenate([q[:, h * HEAD_SIZE : (h + 1) * HEAD_SIZE] for h in range(group)], axis=0)
            scores = lax.dot_general(q, keys, (((1,), (1,)), ((), ())), preferred_element_type=f32)
            probs = []
            for h in range(group):
                head = g * group + h
                sink = sinks[c * kv_heads * group + head]
                sc = jnp.where(allowed, scores[h * WINDOW : (h + 1) * WINDOW] * HEAD_SIZE**-0.5, -jnp.inf)
                top = jnp.maximum(jnp.max(sc, axis=-1, keepdims=True), sink)
                w = jnp.exp(sc - top)
                total = jnp.sum(w, axis=-1, keepdims=True) + jnp.exp(sink - top)
                probs.append((w * (1.0 / total)).astype(jnp.bfloat16))
                logs = jnp.where(lane == head, top + jnp.log(total), logs)
            res = jnp.dot(jnp.concatenate(probs, axis=0), vals, preferred_element_type=f32)
            res = jnp.concatenate([res[h * WINDOW : (h + 1) * WINDOW] for h in range(group)], axis=1)
            mixed[g, pl.ds(base, WINDOW), :] = res.astype(jnp.bfloat16)
        log_out[:, pl.ds(base, WINDOW)] = jnp.transpose(logs)[: kv_heads * group]

    def pool(g):
        @pl.when(has_down)
        def _():
            halo_pool(g).wait_recv()

        index = c * groups + g
        run = pool_ext[g].astype(f32)
        own = run[TILE:]
        trailing = jnp.zeros_like(run)
        span_here = jnp.int32(0)
        reach = 1
        for at, span in enumerate(POOL_SPANS):
            while reach < span:
                run = run + pltpu.roll(run, reach, 0)
                reach *= 2
            trailing = jnp.where(index == at, run, trailing)
            span_here = jnp.where(index == at, span, span_here)
        pos = me * rows + lax.broadcasted_iota(jnp.int32, (rows, 1), 0)
        count = jnp.minimum(pos + 1, span_here).astype(f32)
        centred = (trailing[TILE:] / count - own).astype(jnp.bfloat16)
        product = jnp.dot(centred, mix_own[g], preferred_element_type=f32)
        mixed[kv_heads + g] = (product * pool_gain[index]).astype(jnp.bfloat16)

    n_pairs = out_tiles // 2

    def sum_hop(slot):
        return pltpu.make_async_remote_copy(
            sent.at[slot], got.at[slot], sum_send.at[slot], sum_recv.at[slot],
            device_id={"tp": 1 - c}, device_id_type=MESH_ID,
        )

    def out_project(j, pair):
        slot = j * n_pairs + pair
        acc = None
        for side in range(2):
            first = n_in + 4 * pair + side
            w = jnp.concatenate([held[j, first], held[j, first + 2]], axis=1)
            parts = mixed.shape[0] // 2
            a = jnp.concatenate([mixed[side * parts + i] for i in range(parts)], axis=1)
            term = jnp.dot(a, w, preferred_element_type=f32)
            acc = term if acc is None else acc + term
        low, high = acc[:half], acc[half:]
        mine[slot] = jnp.where(c == 0, low, high)
        sent[slot] = jnp.where(c == 0, high, low)
        sum_hop(slot).start()

    def finish(j, pair):
        slot = j * n_pairs + pair
        sum_hop(slot).wait()
        wide = 2 * LANES
        cols = pl.ds(pl.multiple_of(slot * wide, wide), wide)
        out[:, cols] = (mine[slot] + got[slot]).astype(jnp.bfloat16)

    tasks = {}

    def ready(block):
        return slots.index((block // 3 * CUTS + CUTS - 1, n - 2))

    def at(t, task, *args):
        tasks.setdefault(min(t, len(slots) - 1), []).append((task, args))

    at(-1, norm_all)
    at(ready(1), project_kv)
    for g in range(kv_heads):
        at(ready(2 * g + 3), project_q, g)
    last = ready(2 * kv_heads + 1) + 1
    at(last, kv_arrived)
    for b in range(rows // WINDOW):
        at(last + b // 2, attend, b)
    for g in range(groups):
        at(ready(2 * (1 + kv_heads + g) + 1), project_pool, g)
    for g in range(groups):
        at(ready(2 * (kv_heads + groups) + 1) + (g + 1) // 2, pool, g)
    base_slot = ready(n_in - 1) + 1
    order = []
    for pair in range(n_pairs):
        at(base_slot, out_project, me, pair)
        order.append((base_slot, me, pair))
    for k in range(n - 1):
        for pair in range(n_pairs):
            when = slots.index(((n_in + 4 * pair + 3) // 3 * CUTS + CUTS - 1, k))
            at(max(when, base_slot), out_project, shard[k], pair)
            order.append((max(when, base_slot), shard[k], pair))

    late = []
    for when, j, pair in order:
        if when + 2 < len(slots) - 1:
            at(when + 2, finish, j, pair)
        else:
            late.append((j, pair))
    total_slots = len(slots)
    for t in range(total_slots + Y_LAG):
        if t < total_slots:
            z_step(t)
        if t == X_LAG - 1:
            for task, args in tasks.pop(-1, ()):
                task(*args)
        if 0 <= t - X_LAG < total_slots:
            x_step(t - X_LAG)
        if t >= Y_LAG:
            y_step(t - Y_LAG)
            for task, args in tasks.pop(t - Y_LAG, ()):
                task(*args)
    for j, pair in late:
        finish(j, pair)

    for s in range(steps):
        own_send(s, finish=True)
    for s, k in slots:
        way, more = onward(shard[k])

        @pl.when(more)
        def _():
            z_hop(s, shard[k], way).wait_send()

        x_hop(s, shard[k]).wait_send()
        y_hop(s, shard[k]).wait_send()

    @pl.when(has_up)
    def _():
        halo_kv().wait_send()
        for g in range(groups):
            halo_pool(g).wait_send()


def fused_local(
    n,
    tokens,
    norm_gain,
    query_weight,
    key_matrix,
    value_matrix,
    pool_in_weight,
    head_sink_logit,
    pool_mix,
    pool_gain,
    attn_out_weight,
    pool_out_weight,
):
    _, half, width = tokens.shape
    rows = 2 * half
    depth, q_cols = query_weight.shape
    kv_cols = key_matrix.shape[1]
    pool_cols = pool_in_weight.shape[1]
    heads = q_cols // HEAD_SIZE
    kv_heads = kv_cols // HEAD_SIZE
    groups = pool_cols // POOL_CH
    n_in = (q_cols + 2 * kv_cols + pool_cols) // LANES
    n_blocks = n_in + 2 * attn_out_weight.shape[1] // LANES
    steps = n_blocks // 3 * CUTS
    pieces = n * attn_out_weight.shape[1] // (2 * LANES)
    bf16, f32 = jnp.bfloat16, jnp.float32
    dma = pltpu.SemaphoreType.DMA
    hbm = pl.BlockSpec(memory_space=pl.ANY)
    vmem = pl.BlockSpec(memory_space=pltpu.VMEM)
    smem = pl.BlockSpec(memory_space=pltpu.SMEM)
    mixed, logs = pl.pallas_call(
        functools.partial(layer_kernel, n),
        out_shape=(
            jax.ShapeDtypeStruct((half, width), bf16),
            jax.ShapeDtypeStruct((heads, rows), f32),
        ),
        in_specs=[smem, hbm, vmem, hbm, hbm, hbm, hbm, hbm, vmem, hbm, hbm],
        out_specs=(vmem, vmem),
        scratch_shapes=[
            pltpu.VMEM((n, n_blocks, depth, LANES), bf16),
            pltpu.VMEM((rows, width), bf16),
            pltpu.VMEM((rows, width), bf16),
            pltpu.VMEM((kv_heads, rows, 2 * LANES), bf16),
            pltpu.VMEM((WINDOW + rows, 2 * kv_cols), bf16),
            pltpu.VMEM((groups, TILE + rows, POOL_CH), bf16),
            pltpu.VMEM((kv_heads + groups, rows, 2 * LANES), bf16),
            pltpu.VMEM((groups, POOL_CH, POOL_CH), bf16),
            pltpu.VMEM((pieces, half, 2 * LANES), f32),
            pltpu.VMEM((pieces, half, 2 * LANES), f32),
            pltpu.VMEM((pieces, half, 2 * LANES), f32),
            dma((2, steps, n)),
            dma((steps, n)),
            dma((steps, n)),
            dma((steps, n)),
            dma((steps, n)),
            dma((steps, n)),
            dma((n_blocks,)),
            dma((4,)),
            dma((1 + groups,)),
            dma((1 + groups,)),
            dma((pieces,)),
            dma((pieces,)),
        ],
        compiler_params=pltpu.CompilerParams(
            collective_id=0, has_side_effects=True, vmem_limit_bytes=60 * 1024 * 1024
        ),
    )(
        head_sink_logit,
        tokens[0],
        norm_gain.reshape(1, width),
        query_weight,
        key_matrix,
        value_matrix,
        pool_in_weight,
        pool_mix,
        pool_gain.reshape(-1, 1, POOL_CH),
        attn_out_weight,
        pool_out_weight,
    )
    return mixed[None], logs[None]


def fits(mesh, tokens, query_weight, key_matrix, pool_in_weight, attn_out_weight):
    n, f, c = mesh.shape["sp"], mesh.shape["fs"], mesh.shape["tp"]
    depth = query_weight.shape[0] // n
    rows = tokens.shape[1] // n
    q_cols, kv_cols, pool_cols = (w.shape[1] // c for w in (query_weight, key_matrix, pool_in_weight))
    tiles = attn_out_weight.shape[1] // n // LANES
    blocks = (q_cols + 2 * kv_cols + pool_cols) // LANES + 2 * tiles
    return (
        2 <= n <= 4
        and f == 4
        and c == 2
        and tokens.shape[0] == f
        and rows % WINDOW == 0
        and kv_cols == LANES
        and q_cols == 2 * LANES * (kv_cols // HEAD_SIZE)
        and pool_cols == q_cols
        and POOL_CH == 2 * LANES
        and attn_out_weight.shape[1] % (n * 2 * LANES) == 0
        and attn_out_weight.shape[0] // c == depth
        and depth % LANES == 0
        and blocks % 3 == 0
    )


def solution(mesh):
    in_specs = (
        P("fs", ("sp", "tp"), None),
        P(),
        P("sp", "tp"),
        P("sp", "tp"),
        P("sp", "tp"),
        P("sp", "tp"),
        P(),
        P(),
        P(),
        P("tp", "sp"),
        P("tp", "sp"),
    )
    out_specs = (P("fs", ("sp", "tp"), None), P("fs", "tp", "sp"))

    def step(*args):
        fused = fits(mesh, args[0], args[2], args[3], args[5], args[9])
        body = functools.partial(fused_local, mesh.shape["sp"]) if fused else local
        mapped = jax.shard_map(body, mesh=mesh, in_specs=in_specs, out_specs=out_specs, check_vma=False)
        return mapped(*args)

    return step
```

```python
import functools

import jax
import jax.numpy as jnp
from jax import lax
from jax.experimental import pallas as pl
from jax.experimental.pallas import tpu as pltpu
from jax.sharding import PartitionSpec as P

HEAD_SIZE = 64
WINDOW = 128
POOL_CH = 256


EPSILON = 1e-06
POOL_SPANS = (2, 4, 8, 16)


def passed_along(shard, axis, by):
    size = lax.axis_size(axis)
    pairs = [(i, i + by) for i in range(size) if 0 <= i + by < size]
    return lax.ppermute(shard, axis, pairs)


def windowed_attend(
    query_rows, key_rows, value_rows, key_tail, value_tail, sinks, kv_heads, group, first_pos
):
    rows = query_rows.shape[0]
    blocks = rows // WINDOW
    width = key_rows.shape[1]
    ext_keys = jnp.concatenate([key_tail, key_rows], 0)
    ext_values = jnp.concatenate([value_tail, value_rows], 0)

    def banded(table):
        return jnp.concatenate(
            [
                table[:rows].reshape(blocks, WINDOW, width),
                table[WINDOW:].reshape(blocks, WINDOW, width),
            ],
            axis=1,
        )

    band_keys = banded(ext_keys).reshape(blocks, 2 * WINDOW, kv_heads, HEAD_SIZE)
    band_values = banded(ext_values).reshape(blocks, 2 * WINDOW, kv_heads, HEAD_SIZE)
    query_blocks = query_rows.reshape(blocks, WINDOW, kv_heads, group, HEAD_SIZE)
    scores = jnp.einsum(
        "bqkgd,bskd->bkgqs", query_blocks, band_keys, preferred_element_type=jnp.float32
    ) * HEAD_SIZE ** (-0.5)
    query_pos = first_pos + jnp.arange(rows).reshape(blocks, WINDOW, 1)
    key_pos = (
        first_pos
        - WINDOW
        + jnp.arange(blocks).reshape(blocks, 1, 1) * WINDOW
        + jnp.arange(2 * WINDOW).reshape(1, 1, 2 * WINDOW)
    )
    offset = query_pos - key_pos
    allowed = (offset >= 0) & (offset < WINDOW) & (key_pos >= 0)
    scores = jnp.where(allowed[:, None, None], scores, -jnp.inf)
    sink_grid = sinks.reshape(1, kv_heads, group, 1, 1)
    top = jnp.maximum(jnp.max(scores, axis=-1, keepdims=True), sink_grid)
    weights = jnp.exp(scores - top)
    total = jnp.sum(weights, axis=-1, keepdims=True) + jnp.exp(sink_grid - top)
    probs = (weights / total).astype(jnp.bfloat16)
    mixed = jnp.einsum(
        "bkgqs,bskd->bqkgd", probs, band_values, preferred_element_type=jnp.float32
    ).astype(jnp.bfloat16)
    row_log_weight_sum = (top + jnp.log(total))[..., 0]
    return (
        mixed.reshape(rows, kv_heads * group * HEAD_SIZE),
        row_log_weight_sum.transpose(1, 2, 0, 3).reshape(kv_heads * group, rows),
    )


def pool_branch(pool_rows, pool_tail, mixing, scales, group_start, first_pos):
    rows = pool_rows.shape[0]
    columns = pool_rows.shape[1]
    pool_reach = max(POOL_SPANS)
    extended = jnp.concatenate([pool_tail, pool_rows], 0).astype(jnp.float32)
    group_index = group_start + jnp.arange(columns) // POOL_CH
    span_table = jnp.array(POOL_SPANS, jnp.int32)
    matches = group_index[:, None] == jnp.arange(len(POOL_SPANS))[None, :]
    span_of_col = jnp.sum(jnp.where(matches, span_table[None, :], 0), axis=1)
    trailing = jnp.zeros((rows, columns), jnp.float32)
    for lag in range(pool_reach):
        trailing = trailing + jnp.where(
            lag < span_of_col[None, :], extended[pool_reach - lag : pool_reach - lag + rows], 0.0
        )
    position = first_pos + jnp.arange(rows)
    count = jnp.minimum(position[:, None] + 1, span_of_col[None, :]).astype(jnp.float32)
    centred = (trailing / count - extended[pool_reach:]).astype(jnp.bfloat16)
    grouped = centred.reshape(rows, columns // POOL_CH, POOL_CH)
    product = jnp.einsum(
        "rgc,gcd->rgd", grouped, mixing, preferred_element_type=jnp.float32
    ).reshape(rows, columns)
    return (product * scales).astype(jnp.bfloat16)


def local(
    tokens,
    norm_gain,
    query_weight,
    key_matrix,
    value_matrix,
    pool_in_weight,
    head_sink_logit,
    pool_mix,
    pool_gain,
    attn_out_weight,
    pool_out_weight,
):
    tp_index = lax.axis_index("tp")
    sp_index = lax.axis_index("sp")
    q_cols = query_weight.shape[1]
    kv_cols = key_matrix.shape[1]
    pool_cols = pool_in_weight.shape[1]
    q_heads = q_cols // HEAD_SIZE
    kv_heads = kv_cols // HEAD_SIZE
    groups_dev = pool_cols // POOL_CH
    full_query, full_key, full_value, full_pool = (
        lax.all_gather(query_weight, "sp", axis=0, tiled=True),
        lax.all_gather(key_matrix, "sp", axis=0, tiled=True),
        lax.all_gather(value_matrix, "sp", axis=0, tiled=True),
        lax.all_gather(pool_in_weight, "sp", axis=0, tiled=True),
    )
    values_f = lax.all_gather(tokens[0], "tp", axis=0, tiled=True).astype(jnp.float32)
    scale = lax.rsqrt(jnp.mean(values_f * values_f, axis=-1, keepdims=True) + EPSILON)
    normed = (values_f * scale * norm_gain).astype(jnp.bfloat16)
    outputs = [
        jnp.dot(normed, weight, preferred_element_type=jnp.float32).astype(jnp.bfloat16)
        for weight in (full_query, full_key, full_value, full_pool)
    ]
    projected = jnp.concatenate(outputs, axis=1)
    rows = projected.shape[0]
    first_pos = sp_index * rows
    query_rows = projected[:, :q_cols]
    key_rows = projected[:, q_cols : q_cols + kv_cols]
    value_rows = projected[:, q_cols + kv_cols : q_cols + 2 * kv_cols]
    pool_rows = projected[:, q_cols + 2 * kv_cols :]
    pool_reach = max(POOL_SPANS)
    sinks = lax.dynamic_slice_in_dim(head_sink_logit, tp_index * q_heads, q_heads, 0)
    mixing = lax.dynamic_slice_in_dim(pool_mix, tp_index * groups_dev, groups_dev, 0)
    scales = lax.dynamic_slice_in_dim(pool_gain, tp_index * pool_cols, pool_cols, 0)
    key_tail, value_tail, pool_tail = passed_along(
        (key_rows[rows - WINDOW :], value_rows[rows - WINDOW :], pool_rows[rows - pool_reach :]),
        "sp",
        1,
    )
    attn_part, log_part = windowed_attend(
        query_rows,
        key_rows,
        value_rows,
        key_tail,
        value_tail,
        sinks,
        kv_heads,
        q_heads // kv_heads,
        first_pos,
    )
    pool_part = pool_branch(pool_rows, pool_tail, mixing, scales, tp_index * groups_dev, first_pos)
    half_attn, half_pool = (
        lax.all_gather(attn_out_weight, "sp", axis=1, tiled=True),
        lax.all_gather(pool_out_weight, "sp", axis=1, tiled=True),
    )
    result = lax.psum_scatter(
        jnp.dot(attn_part, half_attn, preferred_element_type=jnp.float32)
        + jnp.dot(pool_part, half_pool, preferred_element_type=jnp.float32),
        "tp",
        scatter_dimension=0,
        tiled=True,
    ).astype(jnp.bfloat16)
    return (result[None], log_part[None])


LANES = 128
TILE = 16
X_LAG, Y_LAG, LEAD = 2,6,1
CUTS, FAR_LAG = 1,0
MESH_ID = pl.DeviceIdType.MESH


def nearest(n, step, me):
    tables = [sorted((j for j in range(n) if j != z), key=lambda j: (abs(j - z), j)) for z in range(n)]
    shard = jnp.int32(tables[0][step])
    for z in range(1, n):
        shard = jnp.where(me == z, tables[z][step], shard)
    return shard


def layer_kernel(
    n,
    sinks,
    tokens,
    gain,
    wq,
    wk,
    wv,
    wp,
    mix,
    pool_gain,
    wao,
    wpo,
    out,
    log_out,
    held,
    tok,
    normed,
    proj,
    kv,
    pool_ext,
    mixed,
    mix_own,
    mine,
    sent,
    got,
    z_send,
    x_send,
    y_send,
    z_recv,
    x_recv,
    y_recv,
    load_sem,
    tok_sem,
    halo_send,
    halo_recv,
    sum_send,
    sum_recv,
):
    me = lax.axis_index("sp")
    f = lax.axis_index("fs")
    c = lax.axis_index("tp")
    f32 = jnp.float32
    half = tokens.shape[0]
    rows = 2 * half
    depth = wq.shape[0]
    n_in = (wq.shape[1] + wk.shape[1] + wv.shape[1] + wp.shape[1]) // LANES
    out_tiles = wao.shape[1] // LANES
    n_blocks = n_in + 2 * out_tiles
    steps = n_blocks // 3 * CUTS
    sources = [wk, wv] + [wq.at[:, pl.ds(i * LANES, LANES)] for i in range(wq.shape[1] // LANES)]
    sources += [wp.at[:, pl.ds(i * LANES, LANES)] for i in range(wp.shape[1] // LANES)]
    for i in range(out_tiles):
        sources += [w.at[:, pl.ds(i * LANES, LANES)] for w in (wao, wpo)]
    z_part = lax.rem(f, 3)
    beside = f + 1 - 2 * lax.rem(f, 2)
    across = lax.rem(f + 2, 4)
    x_part = lax.rem(beside, 3)
    y_part = 3 - z_part - x_part
    relays = (f == 0) | (f == 3)
    y_out = jnp.where(relays, x_part, z_part)
    up, down = me + 1, me - 1
    has_up, has_down = me < n - 1, me > 0

    def load(i):
        return pltpu.make_async_copy(sources[i], held.at[me, i], load_sem.at[i])

    for i in range(n_blocks):
        load(i).start()
    own_rows = pl.ds(pl.multiple_of(c * half, half), half)
    tok_load = pltpu.make_async_copy(tokens, tok.at[own_rows], tok_sem.at[2])
    tok_load.start()
    groups = mix_own.shape[0]
    mix_load = pltpu.make_async_copy(mix.at[pl.ds(c * groups, groups)], mix_own, tok_sem.at[3])
    mix_load.start()

    barrier = pltpu.get_barrier_semaphore()
    pl.semaphore_signal(barrier, inc=1, device_id={"tp": 1 - c}, device_id_type=MESH_ID)
    pl.semaphore_signal(barrier, inc=1, device_id={"fs": beside}, device_id_type=MESH_ID)
    pl.semaphore_signal(barrier, inc=1, device_id={"fs": across}, device_id_type=MESH_ID)

    @pl.when(has_up)
    def _():
        pl.semaphore_signal(barrier, inc=1, device_id={"sp": up}, device_id_type=MESH_ID)

    @pl.when(has_down)
    def _():
        pl.semaphore_signal(barrier, inc=1, device_id={"sp": down}, device_id_type=MESH_ID)

    pl.semaphore_wait(barrier, 3 + has_up.astype(jnp.int32) + has_down.astype(jnp.int32))

    tok_send = pltpu.make_async_remote_copy(
        tokens, tok.at[own_rows], tok_sem.at[0], tok_sem.at[1],
        device_id={"tp": 1 - c}, device_id_type=MESH_ID,
    )
    tok_send.start()

    def hop(s, j, part, send, recv, to):
        size = depth // CUTS
        block = held.at[j, 3 * (s // CUTS) + part, pl.ds(s % CUTS * size, size)]
        return pltpu.make_async_remote_copy(
            block, block, send, recv.at[s, j], device_id=to, device_id_type=MESH_ID
        )

    def z_hop(s, j, way):
        to = jnp.where(way == 0, up, down)
        return hop(s, j, z_part, z_send.at[way, s, j], z_recv, {"sp": to})

    def x_hop(s, j):
        return hop(s, j, z_part, x_send.at[s, j], x_recv, {"fs": beside})

    def y_hop(s, j):
        return hop(s, j, y_out, y_send.at[s, j], y_recv, {"fs": across})

    def onward(j):
        return jnp.where(j < me, 0, 1), ((j < me) & has_up) | ((j > me) & has_down)

    def own_send(s, finish=False):
        @pl.when(has_up)
        def _():
            cp = z_hop(s, me, 0)
            cp.wait_send() if finish else cp.start()

        @pl.when(has_down)
        def _():
            cp = z_hop(s, me, 1)
            cp.wait_send() if finish else cp.start()

    slots = [(s, k) for s in range(steps) for k in range(n - 1)]
    slots.sort(key=lambda slot: (slot[0] + FAR_LAG * slot[1], slot))
    shard = [nearest(n, k, me) for k in range(n - 1)]

    def z_step(t):
        s, k = slots[t]
        j = shard[k]
        if k == 0 and s + LEAD < steps:

            @pl.when(has_up & has_down)
            def _():
                own_send(s + LEAD)

        z_hop(s, j, 0).wait_recv()
        way, more = onward(j)

        @pl.when(more)
        def _():
            z_hop(s, j, way).start()

        x_hop(s, j).start()

        @pl.when(jnp.logical_not(relays))
        def _():
            y_hop(s, j).start()


    def x_step(t):
        s, k = slots[t]
        hop(s, shard[k], x_part, x_send.at[s, shard[k]], x_recv, {"fs": beside}).wait_recv()

        @pl.when(relays)
        def _():
            y_hop(s, shard[k]).start()


    def y_step(t):
        s, k = slots[t]
        hop(s, shard[k], y_part, y_send.at[s, shard[k]], y_recv, {"fs": across}).wait_recv()

    for i in range(n_blocks):
        load(i).wait()
        if i % 3 == 2:
            for s in range(i // 3 * CUTS, (i // 3 + 1) * CUTS):
                if s < LEAD:
                    own_send(s)
                else:

                    @pl.when(jnp.logical_not(has_up & has_down))
                    def _():
                        own_send(s)


    def norm_rows(r, size):
        v = tok[pl.ds(r, size), :].astype(f32)
        scale = lax.rsqrt(jnp.mean(v * v, axis=-1, keepdims=True) + EPSILON)
        normed[pl.ds(r, size), :] = (v * scale * gain[...]).astype(jnp.bfloat16)

    def norm_all():
        tok_load.wait()
        tok_send.wait()
        mix_load.wait()
        chunk = 32

        @pl.loop(0, rows // chunk)
        def _(i):
            norm_rows(pl.multiple_of(i * chunk, chunk), chunk)

    def project(pair):
        acc = None
        for j in range(n):
            w = jnp.concatenate([held[j, 2 * pair], held[j, 2 * pair + 1]], axis=1)
            term = jnp.dot(normed[:, j * depth : (j + 1) * depth], w, preferred_element_type=f32)
            acc = term if acc is None else acc + term
        return acc.astype(jnp.bfloat16)

    def halo_kv():
        return pltpu.make_async_remote_copy(
            kv.at[pl.ds(rows, WINDOW)], kv.at[pl.ds(0, WINDOW)], halo_send.at[0], halo_recv.at[0],
            device_id={"sp": up}, device_id_type=MESH_ID,
        )

    def halo_pool(g):
        return pltpu.make_async_remote_copy(
            pool_ext.at[g, pl.ds(rows, TILE)], pool_ext.at[g, pl.ds(0, TILE)],
            halo_send.at[1 + g], halo_recv.at[1 + g],
            device_id={"sp": up}, device_id_type=MESH_ID,
        )

    def first_zero(store):
        @pl.when(me == 0)
        def _():
            store()

    def project_kv():
        kv[pl.ds(WINDOW, rows), :] = project(0)

        @pl.when(has_up)
        def _():
            halo_kv().start()

        def zero():
            kv[pl.ds(0, WINDOW), :] = jnp.zeros((WINDOW, kv.shape[1]), kv.dtype)

        first_zero(zero)

    def project_q(g):
        proj[g] = project(1 + g)

    kv_cols = wk.shape[1]
    kv_heads = kv_cols // HEAD_SIZE
    group = wq.shape[1] // HEAD_SIZE // kv_heads

    def project_pool(g):
        pool_ext[g, pl.ds(TILE, rows), :] = project(1 + kv_heads + g)

        @pl.when(has_up)
        def _():
            halo_pool(g).start()

        def zero():
            pool_ext[g, pl.ds(0, TILE), :] = jnp.zeros((TILE, POOL_CH), pool_ext.dtype)

        first_zero(zero)

    def kv_arrived():
        @pl.when(has_down)
        def _():
            halo_kv().wait_recv()

    def attend(b):
        base = b * WINDOW
        lane = lax.broadcasted_iota(jnp.int32, (WINDOW, LANES), 1)
        logs = jnp.zeros((WINDOW, LANES), f32)
        i_pos = lax.broadcasted_iota(jnp.int32, (WINDOW, 2 * WINDOW), 0)
        k_pos = lax.broadcasted_iota(jnp.int32, (WINDOW, 2 * WINDOW), 1)
        allowed = (k_pos > i_pos) & (k_pos <= i_pos + WINDOW)
        allowed = allowed & (k_pos + (me * rows + base - WINDOW) >= 0)
        for g in range(kv_heads):
            band = kv[pl.ds(base, 2 * WINDOW), :]
            keys = band[:, g * HEAD_SIZE : (g + 1) * HEAD_SIZE]
            vals = band[:, kv_cols + g * HEAD_SIZE : kv_cols + (g + 1) * HEAD_SIZE]
            q = proj[g, pl.ds(base, WINDOW), :]
            q = jnp.concatenate([q[:, h * HEAD_SIZE : (h + 1) * HEAD_SIZE] for h in range(group)], axis=0)
            scores = lax.dot_general(q, keys, (((1,), (1,)), ((), ())), preferred_element_type=f32)
            probs = []
            for h in range(group):
                head = g * group + h
                sink = sinks[c * kv_heads * group + head]
                sc = jnp.where(allowed, scores[h * WINDOW : (h + 1) * WINDOW] * HEAD_SIZE**-0.5, -jnp.inf)
                top = jnp.maximum(jnp.max(sc, axis=-1, keepdims=True), sink)
                w = jnp.exp(sc - top)
                total = jnp.sum(w, axis=-1, keepdims=True) + jnp.exp(sink - top)
                probs.append((w * (1.0 / total)).astype(jnp.bfloat16))
                logs = jnp.where(lane == head, top + jnp.log(total), logs)
            res = jnp.dot(jnp.concatenate(probs, axis=0), vals, preferred_element_type=f32)
            res = jnp.concatenate([res[h * WINDOW : (h + 1) * WINDOW] for h in range(group)], axis=1)
            mixed[g, pl.ds(base, WINDOW), :] = res.astype(jnp.bfloat16)
        log_out[:, pl.ds(base, WINDOW)] = jnp.transpose(logs)[: kv_heads * group]

    def pool(g):
        @pl.when(has_down)
        def _():
            halo_pool(g).wait_recv()

        index = c * groups + g
        run = pool_ext[g].astype(f32)
        own = run[TILE:]
        trailing = jnp.zeros_like(run)
        span_here = jnp.int32(0)
        reach = 1
        for at, span in enumerate(POOL_SPANS):
            while reach < span:
                run = run + pltpu.roll(run, reach, 0)
                reach *= 2
            trailing = jnp.where(index == at, run, trailing)
            span_here = jnp.where(index == at, span, span_here)
        pos = me * rows + lax.broadcasted_iota(jnp.int32, (rows, 1), 0)
        count = jnp.minimum(pos + 1, span_here).astype(f32)
        centred = (trailing[TILE:] / count - own).astype(jnp.bfloat16)
        product = jnp.dot(centred, mix_own[g], preferred_element_type=f32)
        mixed[kv_heads + g] = (product * pool_gain[index]).astype(jnp.bfloat16)

    n_pairs = out_tiles // 2

    def sum_hop(slot):
        return pltpu.make_async_remote_copy(
            sent.at[slot], got.at[slot], sum_send.at[slot], sum_recv.at[slot],
            device_id={"tp": 1 - c}, device_id_type=MESH_ID,
        )

    def out_project(j, pair):
        slot = j * n_pairs + pair
        acc = None
        for side in range(2):
            first = n_in + 4 * pair + side
            w = jnp.concatenate([held[j, first], held[j, first + 2]], axis=1)
            parts = mixed.shape[0] // 2
            a = jnp.concatenate([mixed[side * parts + i] for i in range(parts)], axis=1)
            term = jnp.dot(a, w, preferred_element_type=f32)
            acc = term if acc is None else acc + term
        low, high = acc[:half], acc[half:]
        mine[slot] = jnp.where(c == 0, low, high)
        sent[slot] = jnp.where(c == 0, high, low)
        sum_hop(slot).start()

    def finish(j, pair):
        slot = j * n_pairs + pair
        sum_hop(slot).wait()
        wide = 2 * LANES
        cols = pl.ds(pl.multiple_of(slot * wide, wide), wide)
        out[:, cols] = (mine[slot] + got[slot]).astype(jnp.bfloat16)

    tasks = {}

    def ready(block):
        return slots.index((block // 3 * CUTS + CUTS - 1, n - 2))

    def at(t, task, *args):
        tasks.setdefault(min(t, len(slots) - 1), []).append((task, args))

    at(-1, norm_all)
    at(ready(1), project_kv)
    for g in range(kv_heads):
        at(ready(2 * g + 3), project_q, g)
    last = ready(2 * kv_heads + 1) + 1
    at(last, kv_arrived)
    for b in range(rows // WINDOW):
        at(last + b // 2, attend, b)
    for g in range(groups):
        at(ready(2 * (1 + kv_heads + g) + 1), project_pool, g)
    for g in range(groups):
        at(ready(2 * (kv_heads + groups) + 1) + (g + 1) // 2, pool, g)
    base_slot = ready(n_in - 1) + 1
    order = []
    for pair in range(n_pairs):
        at(base_slot, out_project, me, pair)
        order.append((base_slot, me, pair))
    for k in range(n - 1):
        for pair in range(n_pairs):
            when = slots.index(((n_in + 4 * pair + 3) // 3 * CUTS + CUTS - 1, k))
            at(max(when, base_slot), out_project, shard[k], pair)
            order.append((max(when, base_slot), shard[k], pair))

    late = []
    for when, j, pair in order:
        if when + 2 < len(slots) - 1:
            at(when + 2, finish, j, pair)
        else:
            late.append((j, pair))
    total_slots = len(slots)
    for t in range(total_slots + Y_LAG):
        if t < total_slots:
            z_step(t)
        if t == X_LAG - 1:
            for task, args in tasks.pop(-1, ()):
                task(*args)
        if 0 <= t - X_LAG < total_slots:
            x_step(t - X_LAG)
        if t >= Y_LAG:
            y_step(t - Y_LAG)
            for task, args in tasks.pop(t - Y_LAG, ()):
                task(*args)
    for j, pair in late:
        finish(j, pair)

    for s in range(steps):
        own_send(s, finish=True)
    for s, k in slots:
        way, more = onward(shard[k])

        @pl.when(more)
        def _():
            z_hop(s, shard[k], way).wait_send()

        x_hop(s, shard[k]).wait_send()
        y_hop(s, shard[k]).wait_send()

    @pl.when(has_up)
    def _():
        halo_kv().wait_send()
        for g in range(groups):
            halo_pool(g).wait_send()


def fused_local(
    n,
    tokens,
    norm_gain,
    query_weight,
    key_matrix,
    value_matrix,
    pool_in_weight,
    head_sink_logit,
    pool_mix,
    pool_gain,
    attn_out_weight,
    pool_out_weight,
):
    _, half, width = tokens.shape
    rows = 2 * half
    depth, q_cols = query_weight.shape
    kv_cols = key_matrix.shape[1]
    pool_cols = pool_in_weight.shape[1]
    heads = q_cols // HEAD_SIZE
    kv_heads = kv_cols // HEAD_SIZE
    groups = pool_cols // POOL_CH
    n_in = (q_cols + 2 * kv_cols + pool_cols) // LANES
    n_blocks = n_in + 2 * attn_out_weight.shape[1] // LANES
    steps = n_blocks // 3 * CUTS
    pieces = n * attn_out_weight.shape[1] // (2 * LANES)
    bf16, f32 = jnp.bfloat16, jnp.float32
    dma = pltpu.SemaphoreType.DMA
    hbm = pl.BlockSpec(memory_space=pl.ANY)
    vmem = pl.BlockSpec(memory_space=pltpu.VMEM)
    smem = pl.BlockSpec(memory_space=pltpu.SMEM)
    mixed, logs = pl.pallas_call(
        functools.partial(layer_kernel, n),
        out_shape=(
            jax.ShapeDtypeStruct((half, width), bf16),
            jax.ShapeDtypeStruct((heads, rows), f32),
        ),
        in_specs=[smem, hbm, vmem, hbm, hbm, hbm, hbm, hbm, vmem, hbm, hbm],
        out_specs=(vmem, vmem),
        scratch_shapes=[
            pltpu.VMEM((n, n_blocks, depth, LANES), bf16),
            pltpu.VMEM((rows, width), bf16),
            pltpu.VMEM((rows, width), bf16),
            pltpu.VMEM((kv_heads, rows, 2 * LANES), bf16),
            pltpu.VMEM((WINDOW + rows, 2 * kv_cols), bf16),
            pltpu.VMEM((groups, TILE + rows, POOL_CH), bf16),
            pltpu.VMEM((kv_heads + groups, rows, 2 * LANES), bf16),
            pltpu.VMEM((groups, POOL_CH, POOL_CH), bf16),
            pltpu.VMEM((pieces, half, 2 * LANES), f32),
            pltpu.VMEM((pieces, half, 2 * LANES), f32),
            pltpu.VMEM((pieces, half, 2 * LANES), f32),
            dma((2, steps, n)),
            dma((steps, n)),
            dma((steps, n)),
            dma((steps, n)),
            dma((steps, n)),
            dma((steps, n)),
            dma((n_blocks,)),
            dma((4,)),
            dma((1 + groups,)),
            dma((1 + groups,)),
            dma((pieces,)),
            dma((pieces,)),
        ],
        compiler_params=pltpu.CompilerParams(
            collective_id=0, has_side_effects=True, vmem_limit_bytes=60 * 1024 * 1024
        ),
    )(
        head_sink_logit,
        tokens[0],
        norm_gain.reshape(1, width),
        query_weight,
        key_matrix,
        value_matrix,
        pool_in_weight,
        pool_mix,
        pool_gain.reshape(-1, 1, POOL_CH),
        attn_out_weight,
        pool_out_weight,
    )
    return mixed[None], logs[None]


def fits(mesh, tokens, query_weight, key_matrix, pool_in_weight, attn_out_weight):
    n, f, c = mesh.shape["sp"], mesh.shape["fs"], mesh.shape["tp"]
    depth = query_weight.shape[0] // n
    rows = tokens.shape[1] // n
    q_cols, kv_cols, pool_cols = (w.shape[1] // c for w in (query_weight, key_matrix, pool_in_weight))
    tiles = attn_out_weight.shape[1] // n // LANES
    blocks = (q_cols + 2 * kv_cols + pool_cols) // LANES + 2 * tiles
    return (
        2 <= n <= 4
        and f == 4
        and c == 2
        and tokens.shape[0] == f
        and rows % WINDOW == 0
        and kv_cols == LANES
        and q_cols == 2 * LANES * (kv_cols // HEAD_SIZE)
        and pool_cols == q_cols
        and POOL_CH == 2 * LANES
        and attn_out_weight.shape[1] % (n * 2 * LANES) == 0
        and attn_out_weight.shape[0] // c == depth
        and depth % LANES == 0
        and blocks % 3 == 0
    )


def solution(mesh):
    in_specs = (
        P("fs", ("sp", "tp"), None),
        P(),
        P("sp", "tp"),
        P("sp", "tp"),
        P("sp", "tp"),
        P("sp", "tp"),
        P(),
        P(),
        P(),
        P("tp", "sp"),
        P("tp", "sp"),
    )
    out_specs = (P("fs", ("sp", "tp"), None), P("fs", "tp", "sp"))

    def step(*args):
        fused = fits(mesh, args[0], args[2], args[3], args[5], args[9])
        body = functools.partial(fused_local, mesh.shape["sp"]) if fused else local
        mapped = jax.shard_map(body, mesh=mesh, in_specs=in_specs, out_specs=out_specs, check_vma=False)
        return mapped(*args)

    return step
```
